32 devices in a mesh: ep: 8 (over z, core), tp: 4 (over y, x).
Axes of the slice: x: 2, y: 2, z: 4, core: 2. Of those that a mesh axis runs over, the one named last changes fastest.
Arguments:
- tokens: bfloat16 [4096, 2048], P(('ep', 'tp')), may hold values from -6 to 6
- routes: int32 [4096, 2], P(('ep', 'tp')), may hold values from 0 to 7, all different within a row; in each aligned block of 128 rows (0 to 127, 128 to 255, ...) at most 48 rows name the same one
- route_weights: float32 [4096, 2], P(('ep', 'tp')), may hold values from 0.25 to 2
- norm_gain: float32 [2048], replicated, may hold values from 0.1 to 1.9
- expert_gate: bfloat16 [8, 2048, 512], P('ep'), may hold values from -0.125 to 0.125
- expert_up: bfloat16 [8, 2048, 512], P('ep'), may hold values from -0.125 to 0.125
- expert_down: bfloat16 [8, 512, 2048], P('ep', None, 'tp')
- shared_gate: bfloat16 [2048, 512], replicated, may hold values from -0.125 to 0.125
- shared_up: bfloat16 [2048, 512], replicated, may hold values from -0.125 to 0.125
- shared_down: bfloat16 [512, 2048], P(None, 'tp')
- out_gain: float32 [2048], P('tp'), may hold values from 0.1 to 1.9
Outputs:
- normalized_out: bfloat16 [4096, 2048], P('ep', 'tp')
The draws below stay inside these ranges and needn't reach their ends.
Inputs may be any that keep to these rules, and one draw needn't show every extreme that they name: `routes`: each row names 2 different experts. Within the rows of one device (aligned blocks of 128 rows) no expert is named by more than 48 rows, a bound that some block reaches.
All inputs are finite; a program needn't handle non-finite values.
Results may differ from the reference program's by a relative error of at most 0.0073.
Values may be sent and summed in bfloat16 or wider, within the bound.
No kernel may reach another device: no remote copies, remote signals or barrier semaphores. Data moves between devices by JAX's collectives and lax.ppermute only.
A program may use at most 64 MiB of HBM per device.

```python
import math
import jax
import jax.numpy as jnp
import numpy as np
from jax import lax

D = 2048
H = 512
TOP_K = 2
TOK_DEV = 128
EXPERTS = 8
CAP = 48
TOKENS = 4096
N_EP = 8
N_TP = 4


def column_scaled(key, shape):
    columns = shape[-1]
    base = jax.random.normal(jax.random.fold_in(key, 11), shape, jnp.float32) * shape[-2] ** (-0.5)
    place = jnp.arange(columns, dtype=jnp.float32) / (columns - 1)
    jitter = jnp.exp(jax.random.uniform(jax.random.fold_in(key, 12), (columns,), jnp.float32, -0.4, 0.4))
    ramp = jnp.exp(0.5 * math.log(3.0) * place)
    factor = ramp * jitter
    factor = factor / jnp.sqrt(jnp.mean(factor * factor))
    return (base * factor).astype(jnp.bfloat16)


def draw_expert_down(key, part):
    return column_scaled(jax.random.fold_in(key, 21), (EXPERTS, H, D))


def draw_shared_down(key, part):
    return column_scaled(jax.random.fold_in(key, 22), (H, D))


def shard_levels(stream_key, dims, shards, least, high):
    level, own = 1.0, jax.random.fold_in(stream_key, 6)
    for axis_at, blocks in shards:
        draws = jnp.exp(jax.random.uniform(jax.random.fold_in(own, axis_at), (blocks,), jnp.float32, least / len(shards), high / len(shards)))
        level = level * jnp.repeat(draws, dims[axis_at] // blocks).reshape([-1 if axis == axis_at else 1 for axis in range(len(dims))])
    return level


def deal_out(rng, own, number, rows, amount, top, limit, lean):
    order = jax.random.permutation(rng, amount)
    crowded, ordinary = portions_of(amount, rows * top, limit, lean, True), portions_of(amount, rows * top, limit, lean, False)
    places = jnp.arange(amount)

    def named(sizes, offset_by):
        used = int((sizes > 0).sum())
        fixed = max(1, used // 4)
        shifted = fixed + (places - fixed + offset_by * (used - fixed)) % max(1, amount - fixed)
        return jnp.zeros((amount,), jnp.int32).at[order[jnp.where(places < fixed, places, shifted)]].set(jnp.asarray(sizes, jnp.int32))

    sizes = jnp.where(number % 4 == 0, named(crowded, number // 4), named(ordinary, number - number // 4 - 1))
    mixed = jax.random.permutation(jax.random.fold_in(own, 3), amount)
    giver, taker = mixed[0:amount // 2 * 2:2], mixed[1:amount // 2 * 2:2]
    margin = jnp.minimum(sizes[giver] - 1, limit - sizes[taker]) // 2
    margin = jnp.where((giver == order[0]) | (taker == order[0]) | (sizes[taker] == 0), 0, jnp.maximum(margin, 0))
    shifted = jax.random.randint(jax.random.fold_in(own, 4), (amount // 2,), 0, 1 << 20) % (margin + 1)
    sizes = sizes.at[giver].add(-shifted).at[taker].add(shifted)
    labels = jnp.searchsorted(jnp.cumsum(sizes), jnp.arange(rows * top), side="right").astype(jnp.int32)
    grid = labels.reshape(top, rows).T
    grid = grid[jax.random.permutation(jax.random.fold_in(own, 1), rows)]
    offset_by = jax.random.randint(jax.random.fold_in(own, 2), (rows, 1), 0, top)
    return jnp.take_along_axis(grid, (jnp.arange(top)[None, :] + offset_by) % top, axis=1)


def portions_of(count, total, most, lean, full):
    loads = [(1 << 20) // math.isqrt(standing ** lean) + 1 for standing in range(1, count + 1)]
    largest = most if full else min(most, max(-(-total // count), total * loads[0] // sum(loads)))
    least = 1 if total - largest >= count - 1 else 0
    holding, rest = [largest] + [least] * (count - 1), total - largest - least * (count - 1)
    while rest > 0:
        movable = [i for i in range(1, count) if holding[i] < largest] or [i for i in range(1, count) if holding[i] < most]
        mass, remaining = sum([loads[i] for i in movable]), rest
        for i in movable:
            addition = min(most - holding[i], max(1, remaining * loads[i] // mass), rest)
            holding[i] = holding[i] + addition
            rest = rest - addition
    return np.array(holding)


def noise(rng, dims, scale, most, cuts=(), held_as=jnp.bfloat16):
    drawn = scale * jax.random.normal(rng, dims, jnp.float32)
    if cuts:
        drawn = drawn * shard_levels(rng, dims, cuts, -0.22, 0.18)
    return jnp.clip(drawn, -most, most).astype(held_as)


def setup_inputs(seed: int = 0) -> dict:
    key_list = jax.random.split(jax.random.key(seed), 12)
    tokens = noise(key_list[0], (TOKENS, D), 1.0, 6.0, ((0, 32),))
    routes_keys = jax.random.split(jax.random.fold_in(key_list[1], 1), TOKENS // TOK_DEV)
    routes_turns = jax.random.permutation(jax.random.fold_in(key_list[1], 3), TOKENS // TOK_DEV)
    routes = jax.vmap(lambda own, number: deal_out(jax.random.fold_in(key_list[1], 2), own, number, TOK_DEV, EXPERTS, TOP_K, CAP, 2))(routes_keys, routes_turns).reshape((TOKENS, TOP_K))
    route_weights = jnp.clip(jnp.exp(math.log(2.0) - 2.0794415 * jax.random.uniform(key_list[2], (TOKENS, TOP_K), jnp.float32) ** shard_levels(key_list[2], (TOKENS, TOP_K), ((0, 32),), -0.2, 0.2)), 0.25, 2.0)
    norm_gain = jnp.clip(1.0 + 0.18 * jax.random.normal(key_list[3], (D,), jnp.float32), 0.1, 1.9)
    expert_gate = noise(key_list[4], (EXPERTS, D, H), D ** -0.5, 0.125, ((0, 8),))
    expert_up = noise(key_list[5], (EXPERTS, D, H), D ** -0.5, 0.125, ((0, 8),))
    expert_down = draw_expert_down(jax.random.fold_in(key_list[11], 71), 0)
    shared_gate = noise(key_list[7], (D, H), D ** -0.5, 0.125)
    shared_up = noise(key_list[8], (D, H), D ** -0.5, 0.125)
    shared_down = draw_shared_down(jax.random.fold_in(key_list[11], 71), 0)
    out_gain = jnp.clip(1.0 + 0.18 * jax.random.normal(key_list[10], (D,), jnp.float32), 0.1, 1.9)
    return dict(tokens=tokens, routes=routes, route_weights=route_weights, norm_gain=norm_gain, expert_gate=expert_gate, expert_up=expert_up, expert_down=expert_down, shared_gate=shared_gate, shared_up=shared_up, shared_down=shared_down, out_gain=out_gain)


def swiglu_rows(rows, gate, upward):
    gate_part = jnp.dot(rows, gate, preferred_element_type=jnp.float32)
    up_part = jnp.dot(rows, upward, preferred_element_type=jnp.float32)
    return (jax.nn.silu(gate_part) * up_part).astype(jnp.bfloat16)

def reference(tokens, routes, route_weights, norm_gain, expert_gate, expert_up, expert_down, shared_gate, shared_up, shared_down, out_gain):
    tokens_f32 = tokens.astype(jnp.float32)
    inverse = lax.rsqrt(lax.optimization_barrier(jnp.mean(tokens_f32 * tokens_f32, axis=1, keepdims=True)) + 1e-06)
    normed = (tokens_f32 * inverse * norm_gain.astype(jnp.float32)[None, :]).astype(jnp.bfloat16)
    shared_hidden = swiglu_rows(normed, shared_gate, shared_up)
    shared_out = jnp.dot(shared_hidden, shared_down, preferred_element_type=jnp.float32)
    most_rows = CAP * N_EP * N_TP

    def add_expert(total, index):
        hits = routes == index
        weight_row = lax.optimization_barrier(jnp.sum(jnp.where(hits, route_weights, jnp.zeros_like(route_weights)), axis=1))
        chosen = jnp.any(hits, axis=1)
        picked = jnp.nonzero(chosen, size=most_rows, fill_value=0)[0].astype(jnp.int32)
        valid = jnp.arange(most_rows, dtype=jnp.int32) < jnp.sum(chosen.astype(jnp.int32))
        rows = normed[picked]
        hidden = swiglu_rows(rows, expert_gate[index], expert_up[index])
        rounded = jnp.dot(hidden, expert_down[index], preferred_element_type=jnp.float32).astype(jnp.bfloat16)
        rounded = lax.optimization_barrier(rounded)
        result = rounded.astype(jnp.float32)
        factor = jnp.where(valid, weight_row[picked], jnp.zeros_like(weight_row[picked]))
        return (total.at[picked].add(result * factor[:, None]), None)
    total, _ = lax.scan(add_expert, shared_out, jnp.arange(EXPERTS, dtype=jnp.int32))
    moe = total.astype(jnp.bfloat16)
    moe = lax.optimization_barrier(moe)
    values = moe.astype(jnp.float32)
    squares = lax.optimization_barrier(jnp.sum(values * values, axis=1, keepdims=True))
    scale = lax.rsqrt(squares / values.shape[1] + 1e-06)
    return (values * scale * out_gain.astype(jnp.float32)[None, :]).astype(jnp.bfloat16)
```

```python
import functools

import jax
import jax.numpy as jnp
from jax import lax
from jax.experimental import pallas as pl
from jax.experimental.pallas import tpu as pltpu
from jax.sharding import PartitionSpec as P


VMEM = pl.BlockSpec(memory_space=pltpu.VMEM)
SMEM = pl.BlockSpec(memory_space=pltpu.SMEM)
F32 = jnp.float32
BF16 = jnp.bfloat16


def dot(a, b):
    return jnp.dot(a, b, preferred_element_type=F32)


def call(kernel, outs, inputs, flops, scalars=0):
    moved = sum(a.size * a.dtype.itemsize for a in inputs)
    moved += sum(o.size * o.dtype.itemsize for o in outs)
    return pl.pallas_call(
        kernel,
        out_shape=outs,
        in_specs=[SMEM] * scalars + [VMEM] * (len(inputs) - scalars),
        out_specs=[VMEM] * len(outs),
        cost_estimate=pl.CostEstimate(flops=flops, bytes_accessed=moved, transcendentals=0),
        compiler_params=pltpu.CompilerParams(vmem_limit_bytes=40 * 1024 * 1024),
    )(*inputs)


def swiglu(rows, gate, upward):
    gate_part = dot(rows, gate)
    up_part = dot(rows, upward)
    return (gate_part / (1.0 + jnp.exp(-gate_part)) * up_part).astype(BF16)


def prepare_kernel(experts, capacity, me, tokens, gain, routes, normed, *pieces):
    values = tokens[...].astype(F32)
    inverse = lax.rsqrt(jnp.mean(values * values, axis=1, keepdims=True) + 1e-06)
    rows = (values * inverse * gain[...]).astype(BF16)
    normed[...] = rows
    count = values.shape[0]
    index = lax.broadcasted_iota(jnp.int32, (experts, count), 0)
    marks = [index == routes[j : j + 1, :] for j in range(routes.shape[0])]
    marked = functools.reduce(jnp.logical_or, marks)
    earlier = lax.broadcasted_iota(jnp.int32, (count, count), 0) < lax.broadcasted_iota(
        jnp.int32, (count, count), 1
    )
    before = dot(marked.astype(BF16), earlier.astype(BF16))
    places = []
    for j, mark in enumerate(marks):
        slot = jnp.sum(jnp.where(mark, before, 0.0), axis=0, keepdims=True)
        places.append((routes[j : j + 1, :] ^ me[0]) * capacity + slot.astype(jnp.int32))
    half = experts // 2
    for start in (half, 0):
        at = lax.broadcasted_iota(jnp.int32, (half * capacity, count), 0) + start * capacity
        chosen = functools.reduce(jnp.logical_or, [at == place for place in places])
        moved = dot(chosen.astype(F32).astype(BF16), rows).astype(BF16)
        for k in range(half):
            pieces[start + k][...] = moved[k * capacity : (k + 1) * capacity]


def table_kernel(experts, capacity, groups, me, *refs):
    packed, outs = refs[: -len(groups)], refs[-len(groups) :]
    for m, ref in enumerate(packed):
        top_count = ref.shape[0] // 2
        count = ref.shape[1]
        columns = [
            jnp.broadcast_to(ref[r : r + 1, :], (count, count)).T for r in range(2 * top_count)
        ]
        lane = lax.broadcasted_iota(jnp.int32, (count, count), 1)
        chosen = [c.astype(jnp.int32) for c in columns[:top_count]]
        marks = [lane == c for c in chosen]
        marked = functools.reduce(jnp.logical_or, marks)
        earlier = lax.broadcasted_iota(jnp.int32, (count, count), 0) > lane
        before = dot(earlier.astype(F32).astype(BF16), marked.astype(F32).astype(BF16))
        places = []
        for c, mark in zip(chosen, marks):
            slot = jnp.sum(jnp.where(mark, before, 0.0), axis=1, keepdims=True)
            places.append((c[:, :1] ^ me[0]) * capacity + slot.astype(jnp.int32))
        for (start, size), out in zip(groups, outs):
            wide = size * capacity
            at = lax.broadcasted_iota(jnp.int32, (count, wide), 1) + start * capacity
            table = functools.reduce(
                jnp.add,
                [
                    jnp.where(at == place, weight[:, :1], 0.0)
                    for place, weight in zip(places, columns[top_count:])
                ],
            )
            for part in range(3):
                piece = table.astype(BF16)
                out[m, part * count : (part + 1) * count, :] = piece
                table = table - piece.astype(F32)


def hidden_kernel(units, shared, *refs):
    rows = jnp.concatenate([r[...] for r in refs[:units]], axis=0)
    gate, upward = refs[units : units + 2]
    out = refs[-1]
    routed = rows.shape[0]
    out[:routed, :] = swiglu(rows, gate[...], upward[...])
    if shared:
        normed, gate, upward = refs[units + 2 : units + 5]
        out[routed:, :] = swiglu(normed[...], gate[...], upward[...])


def down_kernel(blocks, units, capacity, *refs):
    hidden = refs[:blocks]
    down = refs[blocks]
    outs = refs[blocks + 1 :]
    count = units * capacity
    rows = jnp.concatenate([h[:count, :] for h in hidden], axis=0)
    result = dot(rows, down[...]).astype(BF16)
    for u in range(units):
        for m in range(blocks):
            first = m * count + u * capacity
            outs[u][m] = result[first : first + capacity]


def weighted(table, returned, m):
    rows = jnp.concatenate([r[m] for r in returned], axis=0)
    parts = dot(table[m], rows)
    count = parts.shape[0] // 3
    return parts[:count] + parts[count : 2 * count] + parts[2 * count :]


def start_kernel(blocks, units, capacity, *refs):
    hidden = refs[:blocks]
    down, table = refs[blocks : blocks + 2]
    returned = refs[blocks + 2 : blocks + 2 + units]
    out = refs[-1]
    rows = jnp.concatenate([h[units * capacity :, :] for h in hidden], axis=0)
    shared = dot(rows, down[...])
    count = out.shape[1]
    for m in range(blocks):
        out[m] = shared[m * count : (m + 1) * count] + weighted(table, returned, m)


def finish_kernel(blocks, tables, sizes, *refs):
    total = refs[0]
    table = refs[1 : 1 + tables]
    returned = refs[1 + tables : -2]
    moe, squares = refs[-2:]
    ones = jnp.ones((8, moe.shape[2]), F32)
    for m in range(blocks):
        value = total[m]
        first = 0
        for g in range(tables):
            value = value + weighted(table[g], returned[first : first + sizes[g]], m)
            first += sizes[g]
        rounded = value.astype(BF16)
        moe[m] = rounded
        wide = rounded.astype(F32)
        sums = lax.dot_general(
            ones,
            wide * wide,
            (((1,), (1,)), ((), ())),
            precision=lax.Precision.HIGHEST,
            preferred_element_type=F32,
        )
        squares[m : m + 1, :] = sums[:1]


def scale_kernel(blocks, width, me, moe, gain, *refs):
    squares, out = refs[:blocks], refs[-1]
    count = moe.shape[1]
    for m in range(blocks):
        total = squares[0][m : m + 1, :]
        for p in range(1, blocks):
            total = total + squares[p][m ^ p : (m ^ p) + 1, :]
        scale = lax.rsqrt(total / width + 1e-06)
        column = jnp.broadcast_to(scale, (count, count)).T[:, :1]
        first = pl.multiple_of((me[0] ^ m) * count, count)
        value = moe[m].astype(F32) * column * gain[...]
        out[pl.ds(first, count), :] = value.astype(BF16)


def swap(array, axis, k):
    size = lax.axis_size(axis)
    return lax.ppermute(array, axis, [(s, s ^ k) for s in range(size)])


def fast_device(
    tokens,
    routes,
    route_weights,
    norm_gain,
    expert_gate,
    expert_up,
    expert_down,
    shared_gate,
    shared_up,
    shared_down,
    out_gain,
):
    count, width = tokens.shape
    top_count = routes.shape[1]
    experts = lax.axis_size("ep")
    blocks = lax.axis_size("tp")
    inner = expert_gate.shape[2]
    local = expert_down.shape[2]
    capacity = 3 * count * top_count // (2 * experts)
    row = lax.axis_index("ep").astype(jnp.int32).reshape(1)
    column = lax.axis_index("tp").astype(jnp.int32).reshape(1)
    piece = jax.ShapeDtypeStruct((capacity, width), BF16)
    normed, *pieces = call(
        functools.partial(prepare_kernel, experts, capacity),
        [jax.ShapeDtypeStruct((count, width), BF16)] + [piece] * experts,
        [row, tokens, norm_gain[None, :], routes.T],
        2 * experts * capacity * count * width,
        scalars=1,
    )
    half = experts // 2
    arrived = [None] * experts
    for k in list(range(half, experts)) + list(range(1, half)):
        arrived[k] = swap(pieces[k], "ep", k)
    arrived[0] = pieces[0]

    groups = [(0, half), (half, half // 2), (half + half // 2, half // 2)]
    packed = jnp.concatenate([routes.T.astype(F32), route_weights.T], axis=0)
    packed = [packed] + [swap(packed, "tp", m) for m in range(1, blocks)]
    tables = call(
        functools.partial(table_kernel, experts, capacity, groups),
        [jax.ShapeDtypeStruct((blocks, 3 * count, size * capacity), BF16) for _, size in groups],
        [row] + packed,
        blocks * count * count * count,
        scalars=1,
    )

    returned = [None] * experts
    kept = None
    for g, (first, size) in enumerate(groups):
        extra = [normed, shared_gate, shared_up] if g == 0 else []
        rows = size * capacity + (count if g == 0 else 0)
        (hidden,) = call(
            functools.partial(hidden_kernel, size, g == 0),
            [jax.ShapeDtypeStruct((rows, inner), BF16)],
            arrived[first : first + size] + [expert_gate[0], expert_up[0]] + extra,
            4 * rows * width * inner,
        )
        spread = [hidden] + [swap(hidden, "tp", m) for m in range(1, blocks)]
        if g == 0:
            kept = spread
        results = call(
            functools.partial(down_kernel, blocks, size, capacity),
            [jax.ShapeDtypeStruct((blocks, capacity, local), BF16)] * size,
            spread + [expert_down[0]],
            2 * blocks * size * capacity * inner * local,
        )
        for u in range(size):
            k = first + u
            returned[k] = swap(results[u], "ep", k) if k else results[u]

    (total,) = call(
        functools.partial(start_kernel, blocks, half, capacity),
        [jax.ShapeDtypeStruct((blocks, count, local), F32)],
        kept + [shared_down, tables[0]] + returned[:half],
        2 * blocks * count * local * (inner + 3 * half * capacity),
    )
    moe, squares = call(
        functools.partial(finish_kernel, blocks, 2, [size for _, size in groups[1:]]),
        [
            jax.ShapeDtypeStruct((blocks, count, local), BF16),
            jax.ShapeDtypeStruct((blocks, count), F32),
        ],
        [total] + list(tables[1:]) + returned[half:],
        2 * blocks * count * local * 3 * half * capacity,
    )
    squares = [squares] + [swap(squares, "tp", p) for p in range(1, blocks)]
    (out,) = call(
        functools.partial(scale_kernel, blocks, width),
        [jax.ShapeDtypeStruct((blocks * count, local), BF16)],
        [column, moe, out_gain[None, :]] + squares,
        4 * blocks * count * local,
        scalars=1,
    )
    return out


def swiglu_rows(rows, gate, upward):
    gate_part = jnp.dot(rows, gate, preferred_element_type=jnp.float32)
    up_part = jnp.dot(rows, upward, preferred_element_type=jnp.float32)
    return (jax.nn.silu(gate_part) * up_part).astype(jnp.bfloat16)


def plain_device(
    tokens,
    routes,
    route_weights,
    norm_gain,
    expert_gate,
    expert_up,
    expert_down,
    shared_gate,
    shared_up,
    shared_down,
    out_gain,
):
    count_tokens, width = tokens.shape
    top_count = routes.shape[1]
    experts = lax.axis_size("ep")
    capacity = max(2, 3 * count_tokens * top_count // (2 * experts))
    tokens_f32 = tokens.astype(jnp.float32)
    inverse = lax.rsqrt(jnp.mean(tokens_f32 * tokens_f32, axis=1, keepdims=True) + 1e-06)
    normed = (tokens_f32 * inverse * norm_gain[None, :]).astype(jnp.bfloat16)
    chosen = routes.reshape(-1)
    marks = (chosen[:, None] == jnp.arange(experts, dtype=jnp.int32)[None, :]).astype(jnp.int32)
    slots = jnp.sum(jnp.cumsum(marks, axis=0) * marks, axis=1) - 1
    places = chosen * capacity + slots
    owners = jnp.arange(chosen.shape[0], dtype=jnp.int32) // top_count
    table = jnp.zeros((experts * capacity,), jnp.int32).at[places].set(owners)
    filled = jnp.zeros((experts * capacity,), jnp.bool_).at[places].set(True)
    outbound = jnp.where(filled[:, None], normed[table], jnp.zeros((), jnp.bfloat16))
    outbound = outbound.reshape(experts, capacity, width)
    arrived = lax.all_to_all(outbound, "ep", split_axis=0, concat_axis=0, tiled=True).reshape(
        experts * capacity, width
    )
    hidden = swiglu_rows(arrived, expert_gate[0], expert_up[0])
    results = jnp.dot(
        hidden,
        lax.all_gather(expert_down[0], "tp", axis=1, tiled=True),
        preferred_element_type=jnp.float32,
    ).astype(jnp.bfloat16)
    returned = lax.all_to_all(
        results.reshape(experts, capacity, width), "ep", split_axis=0, concat_axis=0, tiled=True
    )
    returned = returned.reshape(experts * capacity, width)
    picked = returned[places].astype(jnp.float32).reshape(count_tokens, top_count, width)
    routed = jnp.sum(picked * route_weights[:, :, None], axis=1)
    shared_hidden = swiglu_rows(normed, shared_gate, shared_up)
    shared_out = jnp.dot(
        shared_hidden,
        lax.all_gather(shared_down, "tp", axis=1, tiled=True),
        preferred_element_type=jnp.float32,
    )
    moe = (shared_out + routed).astype(jnp.bfloat16)
    columns = lax.all_to_all(moe, "tp", split_axis=1, concat_axis=0, tiled=True)
    values = columns.astype(jnp.float32)
    own_rows = moe.astype(jnp.float32)
    totals = lax.all_gather(jnp.sum(own_rows * own_rows, axis=1), "tp", axis=0, tiled=True)
    scale = lax.rsqrt(totals / width + 1e-06)
    return (values * scale[:, None] * out_gain[None, :]).astype(jnp.bfloat16)


def per_device(tokens, routes, *rest):
    count, width = tokens.shape
    experts, blocks = lax.axis_size("ep"), lax.axis_size("tp")
    capacity = 3 * count * routes.shape[1] // (2 * experts)
    powers = experts & (experts - 1) == 0 and blocks & (blocks - 1) == 0
    aligned = capacity % 16 == 0 and width // blocks % 128 == 0 and count % 128 == 0
    fits = powers and aligned and experts >= 8
    return (fast_device if fits else plain_device)(tokens, routes, *rest)


def solution(mesh):
    in_specs = (
        P(("ep", "tp"), None),
        P(("ep", "tp"), None),
        P(("ep", "tp"), None),
        P(),
        P("ep", None, None),
        P("ep", None, None),
        P("ep", None, "tp"),
        P(),
        P(),
        P(None, "tp"),
        P("tp"),
    )
    out_specs = P("ep", "tp")
    return jax.shard_map(
        per_device, mesh=mesh, in_specs=in_specs, out_specs=out_specs, check_vma=False
    )
```

```python
import functools

import jax
import jax.numpy as jnp
from jax import lax
from jax.experimental import pallas as pl
from jax.experimental.pallas import tpu as pltpu
from jax.sharding import PartitionSpec as P


VMEM = pl.BlockSpec(memory_space=pltpu.VMEM)
SMEM = pl.BlockSpec(memory_space=pltpu.SMEM)
HBM = pl.BlockSpec(memory_space=pltpu.HBM)
F32 = jnp.float32
BF16 = jnp.bfloat16


def dot(a, b):
    return jnp.dot(a, b, preferred_element_type=F32)


def call(kernel, outs, inputs, flops, scalars=0, far=(), scratch=()):
    moved = sum(a.size * a.dtype.itemsize for a in inputs)
    moved += sum(o.size * o.dtype.itemsize for o in outs)
    specs = [SMEM] * scalars + [VMEM] * (len(inputs) - scalars)
    for i in far:
        specs[i] = HBM
    return pl.pallas_call(
        kernel,
        out_shape=outs,
        in_specs=specs,
        out_specs=[VMEM] * len(outs),
        scratch_shapes=scratch,
        cost_estimate=pl.CostEstimate(flops=flops, bytes_accessed=moved, transcendentals=0),
        compiler_params=pltpu.CompilerParams(vmem_limit_bytes=40 * 1024 * 1024),
    )(*inputs)


def fetch(sources, targets, sems):
    copies = [
        pltpu.make_async_copy(source, target, sems.at[i])
        for i, (source, target) in enumerate(zip(sources, targets))
    ]
    for copy in copies:
        copy.start()
    return copies


def swiglu(rows, both):
    parts = dot(rows, both)
    inner = parts.shape[1] // 2
    gate_part, up_part = parts[:, :inner], parts[:, inner:]
    return (gate_part / (1.0 + jnp.exp(-gate_part)) * up_part).astype(BF16)


def prepare_kernel(experts, capacity, me, *refs):
    normed, pieces = refs[3], refs[4 : 4 + experts]
    tokens, gain, routes, sems = refs[4 + experts :]
    copies = fetch(refs[:3], (tokens, gain, routes), sems)
    copies[0].wait()
    values = tokens[...].astype(F32)
    inverse = lax.rsqrt(jnp.mean(values * values, axis=1, keepdims=True) + 1e-06)
    copies[1].wait()
    rows = (values * inverse * gain[...]).astype(BF16)
    normed[...] = rows
    copies[2].wait()
    count = values.shape[0]
    index = lax.broadcasted_iota(jnp.int32, (experts, count), 0)
    marks = [index == routes[j : j + 1, :] for j in range(routes.shape[0])]
    marked = functools.reduce(jnp.logical_or, marks)
    earlier = lax.broadcasted_iota(jnp.int32, (count, count), 0) < lax.broadcasted_iota(
        jnp.int32, (count, count), 1
    )
    before = dot(marked.astype(BF16), earlier.astype(BF16))
    places = []
    for j, mark in enumerate(marks):
        slot = jnp.sum(jnp.where(mark, before, 0.0), axis=0, keepdims=True)
        places.append((routes[j : j + 1, :] ^ me[0]) * capacity + slot.astype(jnp.int32))
    half = experts // 2
    for start in (half, 0):
        at = lax.broadcasted_iota(jnp.int32, (half * capacity, count), 0) + start * capacity
        chosen = functools.reduce(jnp.logical_or, [at == place for place in places])
        moved = dot(chosen.astype(F32).astype(BF16), rows).astype(BF16)
        for k in range(half):
            pieces[start + k][...] = moved[k * capacity : (k + 1) * capacity]


def table_kernel(capacity, groups, me, *refs):
    packed, outs = refs[: -len(groups)], refs[-len(groups) :]
    for m, ref in enumerate(packed):
        top_count = ref.shape[0] // 2
        count = ref.shape[1]
        columns = [
            jnp.broadcast_to(ref[r : r + 1, :], (count, count)).T for r in range(2 * top_count)
        ]
        lane = lax.broadcasted_iota(jnp.int32, (count, count), 1)
        chosen = [c.astype(jnp.int32) for c in columns[:top_count]]
        marks = [lane == c for c in chosen]
        marked = functools.reduce(jnp.logical_or, marks)
        earlier = lax.broadcasted_iota(jnp.int32, (count, count), 0) > lane
        before = dot(earlier.astype(F32).astype(BF16), marked.astype(F32).astype(BF16))
        places = []
        for c, mark in zip(chosen, marks):
            slot = jnp.sum(jnp.where(mark, before, 0.0), axis=1, keepdims=True)
            places.append((c[:, :1] ^ me[0]) * capacity + slot.astype(jnp.int32))
        for (start, size), out in zip(groups, outs):
            wide = size * capacity
            at = lax.broadcasted_iota(jnp.int32, (count, wide), 1) + start * capacity
            table = functools.reduce(
                jnp.add,
                [
                    jnp.where(at == place, weight[:, :1], 0.0)
                    for place, weight in zip(places, columns[top_count:])
                ],
            )
            for part in range(3):
                piece = table.astype(BF16)
                out[m, part * count : (part + 1) * count, :] = piece
                table = table - piece.astype(F32)


def stage_kernel(gate, upward, held, both, sems):
    inner = gate.shape[1]
    for copy in fetch((gate, upward), (both.at[:, :inner], both.at[:, inner:]), sems):
        copy.wait()


def shared_kernel(normed, gate, upward, hidden, both, sems):
    inner = gate.shape[1]
    for copy in fetch((gate, upward), (both.at[:, :inner], both.at[:, inner:]), sems):
        copy.wait()
    hidden[...] = swiglu(normed[...], both[...])


def hidden_kernel(*refs):
    rows = jnp.concatenate([r[...] for r in refs[:-2]], axis=0)
    refs[-1][...] = swiglu(rows, refs[-2][...])


def down_kernel(blocks, units, capacity, *refs):
    hidden = refs[:blocks]
    down = refs[blocks]
    outs = refs[blocks + 1 :]
    count = units * capacity
    rows = jnp.concatenate([h[...] for h in hidden], axis=0)
    result = dot(rows, down[...]).astype(BF16)
    for u in range(units):
        for m in range(blocks):
            first = m * count + u * capacity
            outs[u][m] = result[first : first + capacity]


def weighted(table, returned, m):
    rows = jnp.concatenate([r[m] for r in returned], axis=0)
    parts = dot(table[m], rows)
    count = parts.shape[0] // 3
    return parts[:count] + parts[count : 2 * count] + parts[2 * count :]


def base_kernel(blocks, *refs):
    hidden = refs[:blocks]
    down, table = refs[blocks : blocks + 2]
    returned, out = refs[blocks + 2 : -1], refs[-1]
    shared = dot(jnp.concatenate([h[...] for h in hidden], axis=0), down[...])
    count = out.shape[1]
    for m in range(blocks):
        out[m] = shared[m * count : (m + 1) * count] + weighted(table, returned, m)


def more_kernel(blocks, total, table, *refs):
    for m in range(blocks):
        refs[-1][m] = total[m] + weighted(table, refs[:-1], m)


def finish_kernel(blocks, total, table, *refs):
    returned = refs[:-2]
    moe, squares = refs[-2:]
    ones = jnp.ones((8, moe.shape[2]), F32)
    for m in range(blocks):
        rounded = (total[m] + weighted(table, returned, m)).astype(BF16)
        moe[m] = rounded
        wide = rounded.astype(F32)
        sums = lax.dot_general(
            ones,
            wide * wide,
            (((1,), (1,)), ((), ())),
            precision=lax.Precision.HIGHEST,
            preferred_element_type=F32,
        )
        squares[m : m + 1, :] = sums[:1]


def scale_kernel(blocks, width, me, moe, gain, *refs):
    squares, out = refs[:blocks], refs[-1]
    count = moe.shape[1]
    for m in range(blocks):
        total = squares[0][m : m + 1, :]
        for p in range(1, blocks):
            total = total + squares[p][m ^ p : (m ^ p) + 1, :]
        scale = lax.rsqrt(total / width + 1e-06)
        column = jnp.broadcast_to(scale, (count, count)).T[:, :1]
        first = pl.multiple_of((me[0] ^ m) * count, count)
        value = moe[m].astype(F32) * column * gain[...]
        out[pl.ds(first, count), :] = value.astype(BF16)


def swap(array, axis, k):
    size = lax.axis_size(axis)
    return lax.ppermute(array, axis, [(s, s ^ k) for s in range(size)])


def spread(array):
    return [array] + [swap(array, "tp", m) for m in range(1, lax.axis_size("tp"))]


def fast_device(
    tokens,
    routes,
    route_weights,
    norm_gain,
    expert_gate,
    expert_up,
    expert_down,
    shared_gate,
    shared_up,
    shared_down,
    out_gain,
):
    count, width = tokens.shape
    top_count = routes.shape[1]
    experts = lax.axis_size("ep")
    blocks = lax.axis_size("tp")
    inner = expert_gate.shape[2]
    local = expert_down.shape[2]
    capacity = 3 * count * top_count // (2 * experts)
    row = lax.axis_index("ep").astype(jnp.int32).reshape(1)
    column = lax.axis_index("tp").astype(jnp.int32).reshape(1)
    piece = jax.ShapeDtypeStruct((capacity, width), BF16)
    normed, *pieces = call(
        functools.partial(prepare_kernel, experts, capacity),
        [jax.ShapeDtypeStruct((count, width), BF16)] + [piece] * experts,
        [row, tokens, norm_gain[None, :], routes.T],
        2 * experts * capacity * count * width,
        scalars=1,
        far=(1, 2, 3),
        scratch=[
            pltpu.VMEM((count, width), BF16),
            pltpu.VMEM((1, width), F32),
            pltpu.VMEM((top_count, count), jnp.int32),
            pltpu.SemaphoreType.DMA((3,)),
        ],
    )
    half, quarter = experts // 2, experts // 4
    arrived = [pieces[0]] + [swap(pieces[k], "ep", k) for k in range(1, experts)]
    groups = {"N": (0, half), "A": (half, quarter), "B": (half + quarter, quarter)}

    packed = jnp.concatenate([routes.T.astype(F32), route_weights.T], axis=0)
    packed = spread(packed)
    both = jax.ShapeDtypeStruct((width, 2 * inner), BF16)
    (weights,) = call(
        stage_kernel,
        [both],
        [expert_gate[0], expert_up[0], normed],
        count * width,
        far=(0, 1, 2),
        scratch=[pltpu.SemaphoreType.DMA((2,))],
    )
    (shared,) = call(
        shared_kernel,
        [jax.ShapeDtypeStruct((count, inner), BF16)],
        [normed, shared_gate, shared_up],
        4 * count * width * inner,
        far=(1, 2),
        scratch=[pltpu.VMEM(both.shape, BF16), pltpu.SemaphoreType.DMA((2,))],
    )
    shared = spread(shared)
    tables = call(
        functools.partial(table_kernel, capacity, list(groups.values())),
        [
            jax.ShapeDtypeStruct((blocks, 3 * count, size * capacity), BF16)
            for _, size in groups.values()
        ],
        [row] + packed,
        blocks * count * count * count,
        scalars=1,
    )

    returned = {}
    for name, (first, size) in groups.items():
        rows = size * capacity
        (hidden,) = call(
            hidden_kernel,
            [jax.ShapeDtypeStruct((rows, inner), BF16)],
            arrived[first : first + size] + [weights],
            4 * rows * width * inner,
        )
        results = call(
            functools.partial(down_kernel, blocks, size, capacity),
            [jax.ShapeDtypeStruct((blocks, capacity, local), BF16)] * size,
            spread(hidden) + [expert_down[0]],
            2 * blocks * rows * inner * local,
        )
        returned[name] = [
            swap(results[u], "ep", first + u) if first + u else results[u]
            for u in range(size)
        ]

    sums = jax.ShapeDtypeStruct((blocks, count, local), F32)
    (total,) = call(
        functools.partial(base_kernel, blocks),
        [sums],
        shared + [shared_down, tables[0]] + returned["N"],
        2 * blocks * count * local * (inner + 3 * half * capacity),
    )
    (total,) = call(
        functools.partial(more_kernel, blocks),
        [sums],
        [total, tables[1]] + returned["A"],
        2 * blocks * count * local * 3 * quarter * capacity,
    )
    moe, squares = call(
        functools.partial(finish_kernel, blocks),
        [
            jax.ShapeDtypeStruct((blocks, count, local), BF16),
            jax.ShapeDtypeStruct((blocks, count), F32),
        ],
        [total, tables[2]] + returned["B"],
        2 * blocks * count * local * 3 * quarter * capacity,
    )
    (out,) = call(
        functools.partial(scale_kernel, blocks, width),
        [jax.ShapeDtypeStruct((blocks * count, local), BF16)],
        [column, moe, out_gain[None, :]] + spread(squares),
        4 * blocks * count * local,
        scalars=1,
    )
    return out


def swiglu_rows(rows, gate, upward):
    gate_part = jnp.dot(rows, gate, preferred_element_type=jnp.float32)
    up_part = jnp.dot(rows, upward, preferred_element_type=jnp.float32)
    return (jax.nn.silu(gate_part) * up_part).astype(jnp.bfloat16)


def plain_device(
    tokens,
    routes,
    route_weights,
    norm_gain,
    expert_gate,
    expert_up,
    expert_down,
    shared_gate,
    shared_up,
    shared_down,
    out_gain,
):
    count_tokens, width = tokens.shape
    top_count = routes.shape[1]
    experts = lax.axis_size("ep")
    capacity = max(2, 3 * count_tokens * top_count // (2 * experts))
    tokens_f32 = tokens.astype(jnp.float32)
    inverse = lax.rsqrt(jnp.mean(tokens_f32 * tokens_f32, axis=1, keepdims=True) + 1e-06)
    normed = (tokens_f32 * inverse * norm_gain[None, :]).astype(jnp.bfloat16)
    chosen = routes.reshape(-1)
    marks = (chosen[:, None] == jnp.arange(experts, dtype=jnp.int32)[None, :]).astype(jnp.int32)
    slots = jnp.sum(jnp.cumsum(marks, axis=0) * marks, axis=1) - 1
    places = chosen * capacity + slots
    owners = jnp.arange(chosen.shape[0], dtype=jnp.int32) // top_count
    table = jnp.zeros((experts * capacity,), jnp.int32).at[places].set(owners)
    filled = jnp.zeros((experts * capacity,), jnp.bool_).at[places].set(True)
    outbound = jnp.where(filled[:, None], normed[table], jnp.zeros((), jnp.bfloat16))
    outbound = outbound.reshape(experts, capacity, width)
    arrived = lax.all_to_all(outbound, "ep", split_axis=0, concat_axis=0, tiled=True).reshape(
        experts * capacity, width
    )
    hidden = swiglu_rows(arrived, expert_gate[0], expert_up[0])
    results = jnp.dot(
        hidden,
        lax.all_gather(expert_down[0], "tp", axis=1, tiled=True),
        preferred_element_type=jnp.float32,
    ).astype(jnp.bfloat16)
    returned = lax.all_to_all(
        results.reshape(experts, capacity, width), "ep", split_axis=0, concat_axis=0, tiled=True
    )
    returned = returned.reshape(experts * capacity, width)
    picked = returned[places].astype(jnp.float32).reshape(count_tokens, top_count, width)
    routed = jnp.sum(picked * route_weights[:, :, None], axis=1)
    shared_hidden = swiglu_rows(normed, shared_gate, shared_up)
    shared_out = jnp.dot(
        shared_hidden,
        lax.all_gather(shared_down, "tp", axis=1, tiled=True),
        preferred_element_type=jnp.float32,
    )
    moe = (shared_out + routed).astype(jnp.bfloat16)
    columns = lax.all_to_all(moe, "tp", split_axis=1, concat_axis=0, tiled=True)
    values = columns.astype(jnp.float32)
    own_rows = moe.astype(jnp.float32)
    totals = lax.all_gather(jnp.sum(own_rows * own_rows, axis=1), "tp", axis=0, tiled=True)
    scale = lax.rsqrt(totals / width + 1e-06)
    return (values * scale[:, None] * out_gain[None, :]).astype(jnp.bfloat16)


def per_device(tokens, routes, *rest):
    count, width = tokens.shape
    experts, blocks = lax.axis_size("ep"), lax.axis_size("tp")
    capacity = 3 * count * routes.shape[1] // (2 * experts)
    powers = experts & (experts - 1) == 0 and blocks & (blocks - 1) == 0
    aligned = capacity % 16 == 0 and width // blocks % 128 == 0 and count % 128 == 0
    fits = powers and aligned and experts >= 8
    return (fast_device if fits else plain_device)(tokens, routes, *rest)


def solution(mesh):
    in_specs = (
        P(("ep", "tp"), None),
        P(("ep", "tp"), None),
        P(("ep", "tp"), None),
        P(),
        P("ep", None, None),
        P("ep", None, None),
        P("ep", None, "tp"),
        P(),
        P(),
        P(None, "tp"),
        P("tp"),
    )
    out_specs = P("ep", "tp")
    return jax.shard_map(
        per_device, mesh=mesh, in_specs=in_specs, out_specs=out_specs, check_vma=False
    )
```

```python
import functools

import jax
import jax.numpy as jnp
from jax import lax
from jax.experimental import pallas as pl
from jax.experimental.pallas import tpu as pltpu
from jax.sharding import PartitionSpec as P


VMEM = pl.BlockSpec(memory_space=pltpu.VMEM)
SMEM = pl.BlockSpec(memory_space=pltpu.SMEM)
HBM = pl.BlockSpec(memory_space=pltpu.HBM)
F32 = jnp.float32
SPARE = 10800000
BF16 = jnp.bfloat16


def dot(a, b):
    return jnp.dot(a, b, preferred_element_type=F32)


def call(kernel, outs, inputs, flops, scalars=0, far=(), scratch=(), spare=None):
    moved = sum(a.size * a.dtype.itemsize for a in inputs)
    moved += sum(o.size * o.dtype.itemsize for o in outs)
    specs = [SMEM] * scalars + [VMEM] * (len(inputs) - scalars)
    for i in far:
        specs[i] = HBM
    limit = 40 * 1024 * 1024 if spare is None else 67043328 - spare
    return pl.pallas_call(
        kernel,
        out_shape=outs,
        in_specs=specs,
        out_specs=[VMEM] * len(outs),
        scratch_shapes=scratch,
        cost_estimate=pl.CostEstimate(flops=flops, bytes_accessed=moved, transcendentals=0),
        compiler_params=pltpu.CompilerParams(vmem_limit_bytes=limit),
    )(*inputs)


def fetch(sources, targets, sems):
    copies = [
        pltpu.make_async_copy(source, target, sems.at[i])
        for i, (source, target) in enumerate(zip(sources, targets))
    ]
    for copy in copies:
        copy.start()
    return copies


def swiglu(rows, both):
    parts = dot(rows, both)
    inner = parts.shape[1] // 2
    gate_part, up_part = parts[:, :inner], parts[:, inner:]
    return (gate_part / (1.0 + jnp.exp(-gate_part)) * up_part).astype(BF16)


def normalize(values, gain):
    values = values.astype(F32)
    inverse = lax.rsqrt(jnp.mean(values * values, axis=1, keepdims=True) + 1e-06)
    return (values * inverse * gain).astype(BF16)


def prepare_kernel(experts, capacity, me, *refs):
    pieces = refs[2 : 2 + experts]
    tokens, routes, sems = refs[2 + experts :]
    copies = fetch(refs[:2], (tokens, routes), sems)
    copies[1].wait()
    count = tokens.shape[0]
    index = lax.broadcasted_iota(jnp.int32, (experts, count), 0)
    marks = [index == routes[j : j + 1, :] for j in range(routes.shape[0])]
    marked = functools.reduce(jnp.logical_or, marks)
    earlier = lax.broadcasted_iota(jnp.int32, (count, count), 0) < lax.broadcasted_iota(
        jnp.int32, (count, count), 1
    )
    before = dot(marked.astype(BF16), earlier.astype(BF16))
    places = []
    for j, mark in enumerate(marks):
        slot = jnp.sum(jnp.where(mark, before, 0.0), axis=0, keepdims=True)
        places.append((routes[j : j + 1, :] ^ me[0]) * capacity + slot.astype(jnp.int32))
    copies[0].wait()
    rows = tokens[...]
    half = experts // 2
    for start in (half, 0):
        at = lax.broadcasted_iota(jnp.int32, (half * capacity, count), 0) + start * capacity
        chosen = functools.reduce(jnp.logical_or, [at == place for place in places])
        moved = dot(chosen.astype(F32).astype(BF16), rows).astype(BF16)
        for k in range(half):
            pieces[start + k][...] = moved[k * capacity : (k + 1) * capacity]


def table_kernel(capacity, groups, me, *refs):
    packed, outs = refs[: -len(groups)], refs[-len(groups) :]
    for m, ref in enumerate(packed):
        top_count = ref.shape[0] // 2
        count = ref.shape[1]
        columns = [
            jnp.broadcast_to(ref[r : r + 1, :], (count, count)).T for r in range(2 * top_count)
        ]
        lane = lax.broadcasted_iota(jnp.int32, (count, count), 1)
        chosen = [c.astype(jnp.int32) for c in columns[:top_count]]
        marks = [lane == c for c in chosen]
        marked = functools.reduce(jnp.logical_or, marks)
        earlier = lax.broadcasted_iota(jnp.int32, (count, count), 0) > lane
        before = dot(earlier.astype(F32).astype(BF16), marked.astype(F32).astype(BF16))
        places = []
        for c, mark in zip(chosen, marks):
            slot = jnp.sum(jnp.where(mark, before, 0.0), axis=1, keepdims=True)
            places.append((c[:, :1] ^ me[0]) * capacity + slot.astype(jnp.int32))
        for (start, size), out in zip(groups, outs):
            wide = size * capacity
            at = lax.broadcasted_iota(jnp.int32, (count, wide), 1) + start * capacity
            table = functools.reduce(
                jnp.add,
                [
                    jnp.where(at == place, weight[:, :1], 0.0)
                    for place, weight in zip(places, columns[top_count:])
                ],
            )
            for part in range(3):
                piece = table.astype(BF16)
                out[m, part * count : (part + 1) * count, :] = piece
                table = table - piece.astype(F32)


def stage_kernel(gate, upward, held, both, sems):
    inner = gate.shape[1]
    for copy in fetch((gate, upward), (both.at[:, :inner], both.at[:, inner:]), sems):
        copy.wait()


def shared_kernel(tokens, gain, gate, upward, hidden, both, sems):
    inner = gate.shape[1]
    copies = fetch((gate, upward), (both.at[:, :inner], both.at[:, inner:]), sems)
    rows = normalize(tokens[...], gain[...])
    for copy in copies:
        copy.wait()
    hidden[...] = swiglu(rows, both[...])


def hidden_kernel(*refs):
    gain, both, out = refs[-3:]
    rows = jnp.concatenate([r[...] for r in refs[:-3]], axis=0)
    out[...] = swiglu(normalize(rows, gain[...]), both[...])


def down_kernel(blocks, units, capacity, *refs):
    hidden = refs[:blocks]
    down = refs[blocks]
    outs = refs[blocks + 1 :]
    count = units * capacity
    rows = jnp.concatenate([h[...] for h in hidden], axis=0)
    result = dot(rows, down[...]).astype(BF16)
    for u in range(units):
        for m in range(blocks):
            first = m * count + u * capacity
            outs[u][m] = result[first : first + capacity]


def weighted(table, returned, m):
    rows = jnp.concatenate([r[m] for r in returned], axis=0)
    parts = dot(table[m], rows)
    count = parts.shape[0] // 3
    return parts[:count] + parts[count : 2 * count] + parts[2 * count :]


def base_kernel(blocks, *refs):
    hidden = refs[:blocks]
    down, table = refs[blocks : blocks + 2]
    returned, out = refs[blocks + 2 : -1], refs[-1]
    shared = dot(jnp.concatenate([h[...] for h in hidden], axis=0), down[...])
    count = out.shape[1]
    for m in range(blocks):
        out[m] = shared[m * count : (m + 1) * count] + weighted(table, returned, m)


def more_kernel(blocks, total, table, *refs):
    for m in range(blocks):
        refs[-1][m] = total[m] + weighted(table, refs[:-1], m)


def finish_kernel(blocks, lanes, total, table, *refs):
    returned = refs[:-2]
    moe, squares = refs[-2:]
    ones = jnp.ones((8, lanes), F32)
    for m in range(blocks):
        rounded = (total[m] + weighted(table, returned, m)).astype(BF16)
        moe[m] = rounded
        wide = rounded.astype(F32)
        wide = wide * wide
        folded = functools.reduce(
            jnp.add,
            [wide[:, at : at + lanes] for at in range(0, wide.shape[1], lanes)],
        )
        sums = lax.dot_general(
            ones,
            folded,
            (((1,), (1,)), ((), ())),
            precision=lax.Precision.HIGHEST,
            preferred_element_type=F32,
        )
        squares[m : m + 1, :] = sums[:1]


def scale_kernel(blocks, width, me, moe, gain, *refs):
    squares, out = refs[:blocks], refs[-1]
    count = moe.shape[1]
    for m in range(blocks):
        total = squares[0][m : m + 1, :]
        for p in range(1, blocks):
            total = total + squares[p][m ^ p : (m ^ p) + 1, :]
        scale = lax.rsqrt(total / width + 1e-06)
        column = jnp.broadcast_to(scale, (count, count)).T[:, :1]
        first = pl.multiple_of((me[0] ^ m) * count, count)
        value = moe[m].astype(F32) * column * gain[...]
        out[pl.ds(first, count), :] = value.astype(BF16)


def swap(array, axis, k):
    size = lax.axis_size(axis)
    return lax.ppermute(array, axis, [(s, s ^ k) for s in range(size)])


def spread(array):
    return [array] + [swap(array, "tp", m) for m in range(1, lax.axis_size("tp"))]


def fast_device(
    tokens,
    routes,
    route_weights,
    norm_gain,
    expert_gate,
    expert_up,
    expert_down,
    shared_gate,
    shared_up,
    shared_down,
    out_gain,
):
    count, width = tokens.shape
    top_count = routes.shape[1]
    experts = lax.axis_size("ep")
    blocks = lax.axis_size("tp")
    inner = expert_gate.shape[2]
    local = expert_down.shape[2]
    capacity = 3 * count * top_count // (2 * experts)
    row = lax.axis_index("ep").astype(jnp.int32).reshape(1)
    column = lax.axis_index("tp").astype(jnp.int32).reshape(1)
    piece = jax.ShapeDtypeStruct((capacity, width), BF16)
    gain = norm_gain[None, :]
    pieces = call(
        functools.partial(prepare_kernel, experts, capacity),
        [piece] * experts,
        [row, tokens, routes.T],
        2 * experts * capacity * count * width,
        scalars=1,
        far=(1, 2),
        scratch=[
            pltpu.VMEM((count, width), BF16),
            pltpu.VMEM((top_count, count), jnp.int32),
            pltpu.SemaphoreType.DMA((2,)),
        ],
        spare=experts * capacity * width * 2 + SPARE,
    )
    half, quarter = experts // 2, experts // 4
    arrived = [pieces[0]] + [swap(pieces[k], "ep", k) for k in range(1, experts)]
    groups = {"N": (0, half), "A": (half, quarter), "B": (half + quarter, quarter)}

    packed = jnp.concatenate([routes.T.astype(F32), route_weights.T], axis=0)
    packed = spread(packed)
    both = jax.ShapeDtypeStruct((width, 2 * inner), BF16)
    (weights,) = call(
        stage_kernel,
        [both],
        [expert_gate[0], expert_up[0], pieces[0]],
        count * width,
        far=(0, 1, 2),
        scratch=[pltpu.SemaphoreType.DMA((2,))],
    )
    (shared,) = call(
        shared_kernel,
        [jax.ShapeDtypeStruct((count, inner), BF16)],
        [tokens, gain, shared_gate, shared_up],
        4 * count * width * inner,
        far=(2, 3),
        scratch=[pltpu.VMEM(both.shape, BF16), pltpu.SemaphoreType.DMA((2,))],
    )
    shared = spread(shared)
    tables = call(
        functools.partial(table_kernel, capacity, list(groups.values())),
        [
            jax.ShapeDtypeStruct((blocks, 3 * count, size * capacity), BF16)
            for _, size in groups.values()
        ],
        [row] + packed,
        blocks * count * count * count,
        scalars=1,
    )

    returned = {}
    for name, (first, size) in groups.items():
        rows = size * capacity
        (hidden,) = call(
            hidden_kernel,
            [jax.ShapeDtypeStruct((rows, inner), BF16)],
            arrived[first : first + size] + [gain, weights],
            4 * rows * width * inner,
        )
        results = call(
            functools.partial(down_kernel, blocks, size, capacity),
            [jax.ShapeDtypeStruct((blocks, capacity, local), BF16)] * size,
            spread(hidden) + [expert_down[0]],
            2 * blocks * rows * inner * local,
        )
        returned[name] = [
            swap(results[u], "ep", first + u) if first + u else results[u]
            for u in range(size)
        ]

    sums = jax.ShapeDtypeStruct((blocks, count, local), F32)
    (total,) = call(
        functools.partial(base_kernel, blocks),
        [sums],
        shared + [shared_down, tables[0]] + returned["N"],
        2 * blocks * count * local * (inner + 3 * half * capacity),
    )
    (total,) = call(
        functools.partial(more_kernel, blocks),
        [sums],
        [total, tables[1]] + returned["A"],
        2 * blocks * count * local * 3 * quarter * capacity,
    )
    moe, squares = call(
        functools.partial(finish_kernel, blocks, 128),
        [
            jax.ShapeDtypeStruct((blocks, count, local), BF16),
            jax.ShapeDtypeStruct((blocks, count), F32),
        ],
        [total, tables[2]] + returned["B"],
        2 * blocks * count * local * 3 * quarter * capacity,
    )
    (out,) = call(
        functools.partial(scale_kernel, blocks, width),
        [jax.ShapeDtypeStruct((blocks * count, local), BF16)],
        [column, moe, out_gain[None, :]] + spread(squares),
        4 * blocks * count * local,
        scalars=1,
    )
    return out


def swiglu_rows(rows, gate, upward):
    gate_part = jnp.dot(rows, gate, preferred_element_type=jnp.float32)
    up_part = jnp.dot(rows, upward, preferred_element_type=jnp.float32)
    return (jax.nn.silu(gate_part) * up_part).astype(jnp.bfloat16)


def plain_device(
    tokens,
    routes,
    route_weights,
    norm_gain,
    expert_gate,
    expert_up,
    expert_down,
    shared_gate,
    shared_up,
    shared_down,
    out_gain,
):
    count_tokens, width = tokens.shape
    top_count = routes.shape[1]
    experts = lax.axis_size("ep")
    capacity = max(2, 3 * count_tokens * top_count // (2 * experts))
    tokens_f32 = tokens.astype(jnp.float32)
    inverse = lax.rsqrt(jnp.mean(tokens_f32 * tokens_f32, axis=1, keepdims=True) + 1e-06)
    normed = (tokens_f32 * inverse * norm_gain[None, :]).astype(jnp.bfloat16)
    chosen = routes.reshape(-1)
    marks = (chosen[:, None] == jnp.arange(experts, dtype=jnp.int32)[None, :]).astype(jnp.int32)
    slots = jnp.sum(jnp.cumsum(marks, axis=0) * marks, axis=1) - 1
    places = chosen * capacity + slots
    owners = jnp.arange(chosen.shape[0], dtype=jnp.int32) // top_count
    table = jnp.zeros((experts * capacity,), jnp.int32).at[places].set(owners)
    filled = jnp.zeros((experts * capacity,), jnp.bool_).at[places].set(True)
    outbound = jnp.where(filled[:, None], normed[table], jnp.zeros((), jnp.bfloat16))
    outbound = outbound.reshape(experts, capacity, width)
    arrived = lax.all_to_all(outbound, "ep", split_axis=0, concat_axis=0, tiled=True).reshape(
        experts * capacity, width
    )
    hidden = swiglu_rows(arrived, expert_gate[0], expert_up[0])
    results = jnp.dot(
        hidden,
        lax.all_gather(expert_down[0], "tp", axis=1, tiled=True),
        preferred_element_type=jnp.float32,
    ).astype(jnp.bfloat16)
    returned = lax.all_to_all(
        results.reshape(experts, capacity, width), "ep", split_axis=0, concat_axis=0, tiled=True
    )
    returned = returned.reshape(experts * capacity, width)
    picked = returned[places].astype(jnp.float32).reshape(count_tokens, top_count, width)
    routed = jnp.sum(picked * route_weights[:, :, None], axis=1)
    shared_hidden = swiglu_rows(normed, shared_gate, shared_up)
    shared_out = jnp.dot(
        shared_hidden,
        lax.all_gather(shared_down, "tp", axis=1, tiled=True),
        preferred_element_type=jnp.float32,
    )
    moe = (shared_out + routed).astype(jnp.bfloat16)
    columns = lax.all_to_all(moe, "tp", split_axis=1, concat_axis=0, tiled=True)
    values = columns.astype(jnp.float32)
    own_rows = moe.astype(jnp.float32)
    totals = lax.all_gather(jnp.sum(own_rows * own_rows, axis=1), "tp", axis=0, tiled=True)
    scale = lax.rsqrt(totals / width + 1e-06)
    return (values * scale[:, None] * out_gain[None, :]).astype(jnp.bfloat16)


def per_device(tokens, routes, *rest):
    count, width = tokens.shape
    experts, blocks = lax.axis_size("ep"), lax.axis_size("tp")
    capacity = 3 * count * routes.shape[1] // (2 * experts)
    powers = experts & (experts - 1) == 0 and blocks & (blocks - 1) == 0
    aligned = capacity % 16 == 0 and width // blocks % 128 == 0 and count % 128 == 0
    fits = powers and aligned and experts >= 8
    return (fast_device if fits else plain_device)(tokens, routes, *rest)


def solution(mesh):
    in_specs = (
        P(("ep", "tp"), None),
        P(("ep", "tp"), None),
        P(("ep", "tp"), None),
        P(),
        P("ep", None, None),
        P("ep", None, None),
        P("ep", None, "tp"),
        P(),
        P(),
        P(None, "tp"),
        P("tp"),
    )
    out_specs = P("ep", "tp")
    return jax.shard_map(
        per_device, mesh=mesh, in_specs=in_specs, out_specs=out_specs, check_vma=False
    )
```

```python
import functools

import jax
import jax.numpy as jnp
from jax import lax
from jax.experimental import pallas as pl
from jax.experimental.pallas import tpu as pltpu
from jax.sharding import PartitionSpec as P


VMEM = pl.BlockSpec(memory_space=pltpu.VMEM)
SMEM = pl.BlockSpec(memory_space=pltpu.SMEM)
HBM = pl.BlockSpec(memory_space=pltpu.HBM)
F32 = jnp.float32
SPARE = 10800000
BF16 = jnp.bfloat16


def dot(a, b):
    return jnp.dot(a, b, preferred_element_type=F32)


def call(kernel, outs, inputs, flops, scalars=0, far=(), scratch=(), spare=None):
    moved = sum(a.size * a.dtype.itemsize for a in inputs)
    moved += sum(o.size * o.dtype.itemsize for o in outs)
    specs = [SMEM] * scalars + [VMEM] * (len(inputs) - scalars)
    for i in far:
        specs[i] = HBM
    limit = 40 * 1024 * 1024 if spare is None else 67043328 - spare
    return pl.pallas_call(
        kernel,
        out_shape=outs,
        in_specs=specs,
        out_specs=[VMEM] * len(outs),
        scratch_shapes=scratch,
        cost_estimate=pl.CostEstimate(flops=flops, bytes_accessed=moved, transcendentals=0),
        compiler_params=pltpu.CompilerParams(vmem_limit_bytes=limit),
    )(*inputs)


def fetch(sources, targets, sems):
    copies = [
        pltpu.make_async_copy(source, target, sems.at[i])
        for i, (source, target) in enumerate(zip(sources, targets))
    ]
    for copy in copies:
        copy.start()
    return copies


def swiglu(rows, both):
    parts = dot(rows, both)
    inner = parts.shape[1] // 2
    gate_part, up_part = parts[:, :inner], parts[:, inner:]
    return (gate_part / (1.0 + jnp.exp(-gate_part)) * up_part).astype(BF16)


def normalize(values, gain):
    values = values.astype(F32)
    inverse = lax.rsqrt(jnp.mean(values * values, axis=1, keepdims=True) + 1e-06)
    return (values * inverse * gain).astype(BF16)


def compact(me, routes, rows, pieces, capacity, experts):
    count = rows.shape[0]
    index = lax.broadcasted_iota(jnp.int32, (experts, count), 0)
    marks = [index == route for route in routes]
    marked = functools.reduce(jnp.logical_or, marks)
    earlier = lax.broadcasted_iota(jnp.int32, (count, count), 0) < lax.broadcasted_iota(
        jnp.int32, (count, count), 1
    )
    before = dot(marked.astype(BF16), earlier.astype(BF16))
    places = []
    for route, mark in zip(routes, marks):
        slot = jnp.sum(jnp.where(mark, before, 0.0), axis=0, keepdims=True)
        places.append((route ^ me) * capacity + slot.astype(jnp.int32))
    values = rows[...]
    half = experts // 2
    for start in range(len(pieces) - half, -1, -half):
        at = lax.broadcasted_iota(jnp.int32, (half * capacity, count), 0) + start * capacity
        chosen = functools.reduce(jnp.logical_or, [at == place for place in places])
        moved = dot(chosen.astype(F32).astype(BF16), values).astype(BF16)
        for k in range(half):
            pieces[start + k][...] = moved[k * capacity : (k + 1) * capacity]


def prepare_kernel(experts, capacity, me, *refs):
    pieces = refs[2 : 2 + experts]
    tokens, routes, sems = refs[2 + experts :]
    copies = fetch(refs[:2], (tokens, routes), sems)
    for copy in copies:
        copy.wait()
    chosen = [routes[j : j + 1, :] for j in range(routes.shape[0])]
    compact(me[0], chosen, tokens, pieces, capacity, experts)


def relay_kernel(experts, capacity, me, packed, tokens, *pieces):
    chosen = [packed[j : j + 1, :].astype(jnp.int32) for j in range(packed.shape[0] // 2)]
    compact(me[0], chosen, tokens, pieces, capacity, experts)


def table_kernel(capacity, groups, me, *refs):
    packed, outs = refs[: -len(groups)], refs[-len(groups) :]
    for m, ref in enumerate(packed):
        top_count = ref.shape[0] // 2
        count = ref.shape[1]
        columns = [
            jnp.broadcast_to(ref[r : r + 1, :], (count, count)).T for r in range(2 * top_count)
        ]
        lane = lax.broadcasted_iota(jnp.int32, (count, count), 1)
        chosen = [c.astype(jnp.int32) for c in columns[:top_count]]
        marks = [lane == c for c in chosen]
        marked = functools.reduce(jnp.logical_or, marks)
        earlier = lax.broadcasted_iota(jnp.int32, (count, count), 0) > lane
        before = dot(earlier.astype(F32).astype(BF16), marked.astype(F32).astype(BF16))
        places = []
        for c, mark in zip(chosen, marks):
            slot = jnp.sum(jnp.where(mark, before, 0.0), axis=1, keepdims=True)
            places.append((c[:, :1] ^ me[0]) * capacity + slot.astype(jnp.int32))
        for (start, size), out in zip(groups, outs):
            wide = size * capacity
            at = lax.broadcasted_iota(jnp.int32, (count, wide), 1) + start * capacity
            table = functools.reduce(
                jnp.add,
                [
                    jnp.where(at == place, weight[:, :1], 0.0)
                    for place, weight in zip(places, columns[top_count:])
                ],
            )
            for part in range(3):
                piece = table.astype(BF16)
                out[m, part * count : (part + 1) * count, :] = piece
                table = table - piece.astype(F32)


def stage_kernel(gate, upward, held, both, sems):
    inner = gate.shape[1]
    for copy in fetch((gate, upward), (both.at[:, :inner], both.at[:, inner:]), sems):
        copy.wait()


def shared_kernel(tokens, gain, gate, upward, hidden, both, sems):
    inner = gate.shape[1]
    copies = fetch((gate, upward), (both.at[:, :inner], both.at[:, inner:]), sems)
    rows = normalize(tokens[...], gain[...])
    for copy in copies:
        copy.wait()
    hidden[...] = swiglu(rows, both[...])


def joined(refs, ways, at=Ellipsis):
    units = []
    for u in range(0, len(refs), ways):
        units.append(functools.reduce(jnp.add, [r[at] for r in refs[u : u + ways]]))
    return jnp.concatenate(units, axis=0)


def hidden_kernel(ways, *refs):
    gain, both, out = refs[-3:]
    rows = joined(refs[:-3], ways)
    out[...] = swiglu(normalize(rows, gain[...]), both[...])


def down_kernel(blocks, units, capacity, *refs):
    hidden = refs[:blocks]
    down = refs[blocks]
    outs = refs[blocks + 1 :]
    count = units * capacity
    rows = jnp.concatenate([h[...] for h in hidden], axis=0)
    result = dot(rows, down[...]).astype(BF16)
    for u in range(units):
        for m in range(blocks):
            first = m * count + u * capacity
            outs[u][m] = result[first : first + capacity]


def weighted(table, returned, ways, m):
    parts = dot(table[m], joined(returned, ways, m))
    count = parts.shape[0] // 3
    return parts[:count] + parts[count : 2 * count] + parts[2 * count :]


def base_kernel(blocks, *refs):
    hidden = refs[:blocks]
    down, table = refs[blocks : blocks + 2]
    returned, out = refs[blocks + 2 : -1], refs[-1]
    shared = dot(jnp.concatenate([h[...] for h in hidden], axis=0), down[...])
    count = out.shape[1]
    for m in range(blocks):
        out[m] = shared[m * count : (m + 1) * count] + weighted(table, returned, 1, m)


def more_kernel(blocks, total, table, *refs):
    for m in range(blocks):
        refs[-1][m] = total[m] + weighted(table, refs[:-1], 2, m)


def finish_kernel(blocks, lanes, total, table, *refs):
    returned = refs[:-2]
    moe, squares = refs[-2:]
    ones = jnp.ones((8, lanes), F32)
    for m in range(blocks):
        rounded = (total[m] + weighted(table, returned, 2, m)).astype(BF16)
        moe[m] = rounded
        wide = rounded.astype(F32)
        wide = wide * wide
        folded = functools.reduce(
            jnp.add,
            [wide[:, at : at + lanes] for at in range(0, wide.shape[1], lanes)],
        )
        sums = lax.dot_general(
            ones,
            folded,
            (((1,), (1,)), ((), ())),
            precision=lax.Precision.HIGHEST,
            preferred_element_type=F32,
        )
        squares[m : m + 1, :] = sums[:1]


def scale_kernel(blocks, width, me, moe, gain, *refs):
    squares, out = refs[:blocks], refs[-1]
    count = moe.shape[1]
    for m in range(blocks):
        total = squares[0][m : m + 1, :]
        for p in range(1, blocks):
            total = total + squares[p][m ^ p : (m ^ p) + 1, :]
        scale = lax.rsqrt(total / width + 1e-06)
        column = jnp.broadcast_to(scale, (count, count)).T[:, :1]
        first = pl.multiple_of((me[0] ^ m) * count, count)
        value = moe[m].astype(F32) * column * gain[...]
        out[pl.ds(first, count), :] = value.astype(BF16)


def swap(array, axis, k, only=None):
    size = lax.axis_size(axis)
    sources = [s for s in range(size) if only is None or is_inner(s, size) == only]
    return lax.ppermute(array, axis, [(s, s ^ k) for s in sources])


def is_inner(place, size):
    return size // 4 <= place < size - size // 4


def spread(array):
    return [array] + [swap(array, "tp", m) for m in range(1, lax.axis_size("tp"))]


def fast_device(
    tokens,
    routes,
    route_weights,
    norm_gain,
    expert_gate,
    expert_up,
    expert_down,
    shared_gate,
    shared_up,
    shared_down,
    out_gain,
):
    count, width = tokens.shape
    top_count = routes.shape[1]
    experts = lax.axis_size("ep")
    blocks = lax.axis_size("tp")
    inner = expert_gate.shape[2]
    local = expert_down.shape[2]
    capacity = 3 * count * top_count // (2 * experts)
    row = lax.axis_index("ep").astype(jnp.int32).reshape(1)
    column = lax.axis_index("tp").astype(jnp.int32).reshape(1)
    piece = jax.ShapeDtypeStruct((capacity, width), BF16)
    gain = norm_gain[None, :]
    pieces = call(
        functools.partial(prepare_kernel, experts, capacity),
        [piece] * experts,
        [row, tokens, routes.T],
        2 * experts * capacity * count * width,
        scalars=1,
        far=(1, 2),
        scratch=[
            pltpu.VMEM((count, width), BF16),
            pltpu.VMEM((top_count, count), jnp.int32),
            pltpu.SemaphoreType.DMA((2,)),
        ],
        spare=experts * capacity * width * 2 + SPARE,
    )
    half, quarter = experts // 2, experts // 4
    first, last = range(half, half + quarter), range(half + quarter, experts)
    packed = jnp.concatenate([routes.T.astype(F32), route_weights.T], axis=0)
    dense = swap(tokens, "ep", half, only=False)
    dense_routes = swap(packed, "ep", half, only=False)
    near = [pieces[0]] + [swap(pieces[k], "ep", k) for k in range(1, half)]
    direct = {k: swap(pieces[k], "ep", k, only=True) for k in range(half, experts)}
    relayed = call(
        functools.partial(relay_kernel, experts, capacity),
        [piece] * half,
        [row, dense_routes, dense],
        2 * half * capacity * count * width,
        scalars=1,
    )
    passed = [relayed[0]]
    passed += [swap(relayed[k], "ep", k, only=True) for k in range(1, half)]
    arrived = {
        "N": near,
        "A": [direct[k] for u in range(quarter) for k in (last[u], first[u])],
        "B": [passed[k] for u in range(quarter) for k in (u, quarter + u)],
    }
    groups = {"N": (0, half), "A": (half, quarter), "B": (half + quarter, quarter)}
    packed = spread(packed)
    both = jax.ShapeDtypeStruct((width, 2 * inner), BF16)
    (weights,) = call(
        stage_kernel,
        [both],
        [expert_gate[0], expert_up[0], pieces[0]],
        count * width,
        far=(0, 1, 2),
        scratch=[pltpu.SemaphoreType.DMA((2,))],
    )
    (shared,) = call(
        shared_kernel,
        [jax.ShapeDtypeStruct((count, inner), BF16)],
        [tokens, gain, shared_gate, shared_up],
        4 * count * width * inner,
        far=(2, 3),
        scratch=[pltpu.VMEM(both.shape, BF16), pltpu.SemaphoreType.DMA((2,))],
    )
    shared = spread(shared)
    tables = call(
        functools.partial(table_kernel, capacity, list(groups.values())),
        [
            jax.ShapeDtypeStruct((blocks, 3 * count, size * capacity), BF16)
            for _, size in groups.values()
        ],
        [row] + packed,
        blocks * count * count * count,
        scalars=1,
    )

    results = {}
    for name, (_, size) in groups.items():
        rows = size * capacity
        (hidden,) = call(
            functools.partial(hidden_kernel, len(arrived[name]) // size),
            [jax.ShapeDtypeStruct((rows, inner), BF16)],
            arrived[name] + [gain, weights],
            4 * rows * width * inner,
        )
        results[name] = call(
            functools.partial(down_kernel, blocks, size, capacity),
            [jax.ShapeDtypeStruct((blocks, capacity, local), BF16)] * size,
            spread(hidden) + [expert_down[0]],
            2 * blocks * rows * inner * local,
        )
    returned = {"N": [results["N"][0]], "A": [], "B": []}
    for k in range(1, half):
        returned["N"].append(swap(results["N"][k], "ep", k))
    for u in range(quarter):
        for name, k in (("A", first[u]), ("B", last[u])):
            for phase in "AB":
                only = (phase == "A") == (name == "B")
                returned[name].append(swap(results[phase][u], "ep", k, only=only))

    sums = jax.ShapeDtypeStruct((blocks, count, local), F32)
    (total,) = call(
        functools.partial(base_kernel, blocks),
        [sums],
        shared + [shared_down, tables[0]] + returned["N"],
        2 * blocks * count * local * (inner + 3 * half * capacity),
    )
    (total,) = call(
        functools.partial(more_kernel, blocks),
        [sums],
        [total, tables[1]] + returned["A"],
        2 * blocks * count * local * 3 * quarter * capacity,
    )
    moe, squares = call(
        functools.partial(finish_kernel, blocks, 128),
        [
            jax.ShapeDtypeStruct((blocks, count, local), BF16),
            jax.ShapeDtypeStruct((blocks, count), F32),
        ],
        [total, tables[2]] + returned["B"],
        2 * blocks * count * local * 3 * quarter * capacity,
    )
    (out,) = call(
        functools.partial(scale_kernel, blocks, width),
        [jax.ShapeDtypeStruct((blocks * count, local), BF16)],
        [column, moe, out_gain[None, :]] + spread(squares),
        4 * blocks * count * local,
        scalars=1,
    )
    return out


def swiglu_rows(rows, gate, upward):
    gate_part = jnp.dot(rows, gate, preferred_element_type=jnp.float32)
    up_part = jnp.dot(rows, upward, preferred_element_type=jnp.float32)
    return (jax.nn.silu(gate_part) * up_part).astype(jnp.bfloat16)


def plain_device(
    tokens,
    routes,
    route_weights,
    norm_gain,
    expert_gate,
    expert_up,
    expert_down,
    shared_gate,
    shared_up,
    shared_down,
    out_gain,
):
    count_tokens, width = tokens.shape
    top_count = routes.shape[1]
    experts = lax.axis_size("ep")
    capacity = max(2, 3 * count_tokens * top_count // (2 * experts))
    tokens_f32 = tokens.astype(jnp.float32)
    inverse = lax.rsqrt(jnp.mean(tokens_f32 * tokens_f32, axis=1, keepdims=True) + 1e-06)
    normed = (tokens_f32 * inverse * norm_gain[None, :]).astype(jnp.bfloat16)
    chosen = routes.reshape(-1)
    marks = (chosen[:, None] == jnp.arange(experts, dtype=jnp.int32)[None, :]).astype(jnp.int32)
    slots = jnp.sum(jnp.cumsum(marks, axis=0) * marks, axis=1) - 1
    places = chosen * capacity + slots
    owners = jnp.arange(chosen.shape[0], dtype=jnp.int32) // top_count
    table = jnp.zeros((experts * capacity,), jnp.int32).at[places].set(owners)
    filled = jnp.zeros((experts * capacity,), jnp.bool_).at[places].set(True)
    outbound = jnp.where(filled[:, None], normed[table], jnp.zeros((), jnp.bfloat16))
    outbound = outbound.reshape(experts, capacity, width)
    arrived = lax.all_to_all(outbound, "ep", split_axis=0, concat_axis=0, tiled=True).reshape(
        experts * capacity, width
    )
    hidden = swiglu_rows(arrived, expert_gate[0], expert_up[0])
    results = jnp.dot(
        hidden,
        lax.all_gather(expert_down[0], "tp", axis=1, tiled=True),
        preferred_element_type=jnp.float32,
    ).astype(jnp.bfloat16)
    returned = lax.all_to_all(
        results.reshape(experts, capacity, width), "ep", split_axis=0, concat_axis=0, tiled=True
    )
    returned = returned.reshape(experts * capacity, width)
    picked = returned[places].astype(jnp.float32).reshape(count_tokens, top_count, width)
    routed = jnp.sum(picked * route_weights[:, :, None], axis=1)
    shared_hidden = swiglu_rows(normed, shared_gate, shared_up)
    shared_out = jnp.dot(
        shared_hidden,
        lax.all_gather(shared_down, "tp", axis=1, tiled=True),
        preferred_element_type=jnp.float32,
    )
    moe = (shared_out + routed).astype(jnp.bfloat16)
    columns = lax.all_to_all(moe, "tp", split_axis=1, concat_axis=0, tiled=True)
    values = columns.astype(jnp.float32)
    own_rows = moe.astype(jnp.float32)
    totals = lax.all_gather(jnp.sum(own_rows * own_rows, axis=1), "tp", axis=0, tiled=True)
    scale = lax.rsqrt(totals / width + 1e-06)
    return (values * scale[:, None] * out_gain[None, :]).astype(jnp.bfloat16)


def per_device(tokens, routes, *rest):
    count, width = tokens.shape
    experts, blocks = lax.axis_size("ep"), lax.axis_size("tp")
    capacity = 3 * count * routes.shape[1] // (2 * experts)
    powers = experts & (experts - 1) == 0 and blocks & (blocks - 1) == 0
    aligned = capacity % 16 == 0 and width // blocks % 128 == 0 and count % 128 == 0
    fits = powers and aligned and experts >= 8
    return (fast_device if fits else plain_device)(tokens, routes, *rest)


def solution(mesh):
    in_specs = (
        P(("ep", "tp"), None),
        P(("ep", "tp"), None),
        P(("ep", "tp"), None),
        P(),
        P("ep", None, None),
        P("ep", None, None),
        P("ep", None, "tp"),
        P(),
        P(),
        P(None, "tp"),
        P("tp"),
    )
    out_specs = P("ep", "tp")
    return jax.shard_map(
        per_device, mesh=mesh, in_specs=in_specs, out_specs=out_specs, check_vma=False
    )
```

```python
import functools

import jax
import jax.numpy as jnp
from jax import lax
from jax.experimental import pallas as pl
from jax.experimental.pallas import tpu as pltpu
from jax.sharding import PartitionSpec as P


VMEM = pl.BlockSpec(memory_space=pltpu.VMEM)
SMEM = pl.BlockSpec(memory_space=pltpu.SMEM)
HBM = pl.BlockSpec(memory_space=pltpu.HBM)
F32 = jnp.float32
SPARE = 10800000
BF16 = jnp.bfloat16


def dot(a, b):
    return jnp.dot(a, b, preferred_element_type=F32)


def call(kernel, outs, inputs, flops, scalars=0, far=(), scratch=(), spare=None, far_out=False):
    moved = sum(a.size * a.dtype.itemsize for a in inputs)
    moved += sum(o.size * o.dtype.itemsize for o in outs)
    specs = [SMEM] * scalars + [VMEM] * (len(inputs) - scalars)
    for i in far:
        specs[i] = HBM
    limit = 40 * 1024 * 1024 if spare is None else 67043328 - spare
    return pl.pallas_call(
        kernel,
        out_shape=outs,
        in_specs=specs,
        out_specs=[HBM if far_out else VMEM] * len(outs),
        scratch_shapes=scratch,
        cost_estimate=pl.CostEstimate(flops=flops, bytes_accessed=moved, transcendentals=0),
        compiler_params=pltpu.CompilerParams(vmem_limit_bytes=limit),
    )(*inputs)


def fetch(sources, targets, sems):
    copies = [
        pltpu.make_async_copy(source, target, sems.at[i])
        for i, (source, target) in enumerate(zip(sources, targets))
    ]
    for copy in copies:
        copy.start()
    return copies


def swiglu(rows, both):
    parts = dot(rows, both)
    inner = parts.shape[1] // 2
    gate_part, up_part = parts[:, :inner], parts[:, inner:]
    return (gate_part / (1.0 + jnp.exp(-gate_part)) * up_part).astype(BF16)


def normalize(values, gain):
    values = values.astype(F32)
    inverse = lax.rsqrt(jnp.mean(values * values, axis=1, keepdims=True) + 1e-06)
    return (values * inverse * gain).astype(BF16)


def prepare_kernel(experts, capacity, me, *refs):
    pieces = refs[2 : 2 + experts]
    tokens, routes, sems = refs[2 + experts :]
    copies = fetch(refs[:2], (tokens, routes), sems)
    copies[1].wait()
    count = tokens.shape[0]
    index = lax.broadcasted_iota(jnp.int32, (experts, count), 0)
    marks = [index == routes[j : j + 1, :] for j in range(routes.shape[0])]
    marked = functools.reduce(jnp.logical_or, marks)
    earlier = lax.broadcasted_iota(jnp.int32, (count, count), 0) < lax.broadcasted_iota(
        jnp.int32, (count, count), 1
    )
    before = dot(marked.astype(BF16), earlier.astype(BF16))
    places = []
    for j, mark in enumerate(marks):
        slot = jnp.sum(jnp.where(mark, before, 0.0), axis=0, keepdims=True)
        places.append((routes[j : j + 1, :] ^ me[0]) * capacity + slot.astype(jnp.int32))
    copies[0].wait()
    rows = tokens[...]
    half = experts // 2
    for start in (half, 0):
        at = lax.broadcasted_iota(jnp.int32, (half * capacity, count), 0) + start * capacity
        chosen = functools.reduce(jnp.logical_or, [at == place for place in places])
        moved = dot(chosen.astype(F32).astype(BF16), rows).astype(BF16)
        for k in range(half):
            pieces[start + k][...] = moved[k * capacity : (k + 1) * capacity]


def table_kernel(capacity, groups, me, *refs):
    packed, outs = refs[: -len(groups)], refs[-len(groups) :]
    for m, ref in enumerate(packed):
        top_count = ref.shape[0] // 2
        count = ref.shape[1]
        columns = [
            jnp.broadcast_to(ref[r : r + 1, :], (count, count)).T for r in range(2 * top_count)
        ]
        lane = lax.broadcasted_iota(jnp.int32, (count, count), 1)
        chosen = [c.astype(jnp.int32) for c in columns[:top_count]]
        marks = [lane == c for c in chosen]
        marked = functools.reduce(jnp.logical_or, marks)
        earlier = lax.broadcasted_iota(jnp.int32, (count, count), 0) > lane
        before = dot(earlier.astype(F32).astype(BF16), marked.astype(F32).astype(BF16))
        places = []
        for c, mark in zip(chosen, marks):
            slot = jnp.sum(jnp.where(mark, before, 0.0), axis=1, keepdims=True)
            places.append((c[:, :1] ^ me[0]) * capacity + slot.astype(jnp.int32))
        for (start, size), out in zip(groups, outs):
            wide = size * capacity
            at = lax.broadcasted_iota(jnp.int32, (count, wide), 1) + start * capacity
            table = functools.reduce(
                jnp.add,
                [
                    jnp.where(at == place, weight[:, :1], 0.0)
                    for place, weight in zip(places, columns[top_count:])
                ],
            )
            for part in range(3):
                piece = table.astype(BF16)
                out[m, part * count : (part + 1) * count, :] = piece
                table = table - piece.astype(F32)


def stage_kernel(gate, upward, held, both, sems):
    inner = gate.shape[1]
    for copy in fetch((gate, upward), (both.at[:, :inner], both.at[:, inner:]), sems):
        copy.wait()


def shared_kernel(tokens, gain, gate, upward, hidden, both, sems):
    inner = gate.shape[1]
    copies = fetch((gate, upward), (both.at[:, :inner], both.at[:, inner:]), sems)
    rows = normalize(tokens[...], gain[...])
    for copy in copies:
        copy.wait()
    hidden[...] = swiglu(rows, both[...])


def hidden_kernel(*refs):
    gain, both, out = refs[-3:]
    rows = jnp.concatenate([r[...] for r in refs[:-3]], axis=0)
    out[...] = swiglu(normalize(rows, gain[...]), both[...])


def down_kernel(blocks, units, capacity, *refs):
    hidden = refs[:blocks]
    down = refs[blocks]
    outs = refs[blocks + 1 :]
    count = units * capacity
    rows = jnp.concatenate([h[...] for h in hidden], axis=0)
    result = dot(rows, down[...]).astype(BF16)
    for u in range(units):
        for m in range(blocks):
            first = m * count + u * capacity
            outs[u][m] = result[first : first + capacity]


def weighted(table, returned, m):
    rows = jnp.concatenate([r[m] for r in returned], axis=0)
    parts = dot(table[m], rows)
    count = parts.shape[0] // 3
    return parts[:count] + parts[count : 2 * count] + parts[2 * count :]


def base_kernel(blocks, *refs):
    hidden = refs[:blocks]
    down, table = refs[blocks : blocks + 2]
    returned, out = refs[blocks + 2 : -1], refs[-1]
    shared = dot(jnp.concatenate([h[...] for h in hidden], axis=0), down[...])
    count = out.shape[1]
    for m in range(blocks):
        out[m] = shared[m * count : (m + 1) * count] + weighted(table, returned, m)


def more_kernel(blocks, total, table, *refs):
    for m in range(blocks):
        refs[-1][m] = total[m] + weighted(table, refs[:-1], m)


def finish_kernel(blocks, lanes, total, table, *refs):
    returned = refs[:-2]
    moe, squares = refs[-2:]
    ones = jnp.ones((8, lanes), F32)
    for m in range(blocks):
        rounded = (total[m] + weighted(table, returned, m)).astype(BF16)
        moe[m] = rounded
        wide = rounded.astype(F32)
        wide = wide * wide
        folded = functools.reduce(
            jnp.add,
            [wide[:, at : at + lanes] for at in range(0, wide.shape[1], lanes)],
        )
        sums = lax.dot_general(
            ones,
            folded,
            (((1,), (1,)), ((), ())),
            precision=lax.Precision.HIGHEST,
            preferred_element_type=F32,
        )
        squares[m : m + 1, :] = sums[:1]


def scale_kernel(blocks, width, me, moe, gain, *refs):
    squares, out, ready, sems = refs[:blocks], *refs[blocks:]
    count = moe.shape[1]
    copies = []
    for m in range(blocks):
        total = squares[0][m : m + 1, :]
        for p in range(1, blocks):
            total = total + squares[p][m ^ p : (m ^ p) + 1, :]
        scale = lax.rsqrt(total / width + 1e-06)
        column = jnp.broadcast_to(scale, (count, count)).T[:, :1]
        ready[m] = (moe[m].astype(F32) * column * gain[...]).astype(BF16)
        first = pl.multiple_of((me[0] ^ m) * count, count)
        copy = pltpu.make_async_copy(ready.at[m], out.at[pl.ds(first, count), :], sems.at[m])
        copy.start()
        copies.append(copy)
    for copy in copies:
        copy.wait()


def swap(array, axis, k):
    size = lax.axis_size(axis)
    return lax.ppermute(array, axis, [(s, s ^ k) for s in range(size)])


def spread(array):
    return [array] + [swap(array, "tp", m) for m in range(1, lax.axis_size("tp"))]


def fast_device(
    tokens,
    routes,
    route_weights,
    norm_gain,
    expert_gate,
    expert_up,
    expert_down,
    shared_gate,
    shared_up,
    shared_down,
    out_gain,
):
    count, width = tokens.shape
    top_count = routes.shape[1]
    experts = lax.axis_size("ep")
    blocks = lax.axis_size("tp")
    inner = expert_gate.shape[2]
    local = expert_down.shape[2]
    capacity = 3 * count * top_count // (2 * experts)
    row = lax.axis_index("ep").astype(jnp.int32).reshape(1)
    column = lax.axis_index("tp").astype(jnp.int32).reshape(1)
    piece = jax.ShapeDtypeStruct((capacity, width), BF16)
    gain = norm_gain[None, :]
    pieces = call(
        functools.partial(prepare_kernel, experts, capacity),
        [piece] * experts,
        [row, tokens, routes.T],
        2 * experts * capacity * count * width,
        scalars=1,
        far=(1, 2),
        scratch=[
            pltpu.VMEM((count, width), BF16),
            pltpu.VMEM((top_count, count), jnp.int32),
            pltpu.SemaphoreType.DMA((2,)),
        ],
        spare=experts * capacity * width * 2 + SPARE,
    )
    half, quarter = experts // 2, experts // 4
    arrived = [pieces[0]] + [swap(pieces[k], "ep", k) for k in range(1, experts)]
    groups = {"N": (0, half), "A": (half + quarter, quarter), "B": (half, quarter)}

    packed = jnp.concatenate([routes.T.astype(F32), route_weights.T], axis=0)
    packed = spread(packed)
    both = jax.ShapeDtypeStruct((width, 2 * inner), BF16)
    (weights,) = call(
        stage_kernel,
        [both],
        [expert_gate[0], expert_up[0], pieces[0]],
        count * width,
        far=(0, 1, 2),
        scratch=[pltpu.SemaphoreType.DMA((2,))],
    )
    (shared,) = call(
        shared_kernel,
        [jax.ShapeDtypeStruct((count, inner), BF16)],
        [tokens, gain, shared_gate, shared_up],
        4 * count * width * inner,
        far=(2, 3),
        scratch=[pltpu.VMEM(both.shape, BF16), pltpu.SemaphoreType.DMA((2,))],
    )
    shared = spread(shared)
    tables = call(
        functools.partial(table_kernel, capacity, list(groups.values())),
        [
            jax.ShapeDtypeStruct((blocks, 3 * count, size * capacity), BF16)
            for _, size in groups.values()
        ],
        [row] + packed,
        blocks * count * count * count,
        scalars=1,
    )

    returned = {}
    for name, (first, size) in groups.items():
        rows = size * capacity
        (hidden,) = call(
            hidden_kernel,
            [jax.ShapeDtypeStruct((rows, inner), BF16)],
            arrived[first : first + size] + [gain, weights],
            4 * rows * width * inner,
        )
        results = call(
            functools.partial(down_kernel, blocks, size, capacity),
            [jax.ShapeDtypeStruct((blocks, capacity, local), BF16)] * size,
            spread(hidden) + [expert_down[0]],
            2 * blocks * rows * inner * local,
        )
        returned[name] = [
            swap(results[u], "ep", first + u) if first + u else results[u]
            for u in range(size)
        ]

    sums = jax.ShapeDtypeStruct((blocks, count, local), F32)
    (total,) = call(
        functools.partial(base_kernel, blocks),
        [sums],
        shared + [shared_down, tables[0]] + returned["N"],
        2 * blocks * count * local * (inner + 3 * half * capacity),
    )
    (total,) = call(
        functools.partial(more_kernel, blocks),
        [sums],
        [total, tables[1]] + returned["A"],
        2 * blocks * count * local * 3 * quarter * capacity,
    )
    moe, squares = call(
        functools.partial(finish_kernel, blocks, 128),
        [
            jax.ShapeDtypeStruct((blocks, count, local), BF16),
            jax.ShapeDtypeStruct((blocks, count), F32),
        ],
        [total, tables[2]] + returned["B"],
        2 * blocks * count * local * 3 * quarter * capacity,
    )
    (out,) = call(
        functools.partial(scale_kernel, blocks, width),
        [jax.ShapeDtypeStruct((blocks * count, local), BF16)],
        [column, moe, out_gain[None, :]] + spread(squares),
        4 * blocks * count * local,
        scalars=1,
        scratch=[
            pltpu.VMEM((blocks, count, local), BF16),
            pltpu.SemaphoreType.DMA((blocks,)),
        ],
        far_out=True,
    )
    return out


def swiglu_rows(rows, gate, upward):
    gate_part = jnp.dot(rows, gate, preferred_element_type=jnp.float32)
    up_part = jnp.dot(rows, upward, preferred_element_type=jnp.float32)
    return (jax.nn.silu(gate_part) * up_part).astype(jnp.bfloat16)


def plain_device(
    tokens,
    routes,
    route_weights,
    norm_gain,
    expert_gate,
    expert_up,
    expert_down,
    shared_gate,
    shared_up,
    shared_down,
    out_gain,
):
    count_tokens, width = tokens.shape
    top_count = routes.shape[1]
    experts = lax.axis_size("ep")
    capacity = max(2, 3 * count_tokens * top_count // (2 * experts))
    tokens_f32 = tokens.astype(jnp.float32)
    inverse = lax.rsqrt(jnp.mean(tokens_f32 * tokens_f32, axis=1, keepdims=True) + 1e-06)
    normed = (tokens_f32 * inverse * norm_gain[None, :]).astype(jnp.bfloat16)
    chosen = routes.reshape(-1)
    marks = (chosen[:, None] == jnp.arange(experts, dtype=jnp.int32)[None, :]).astype(jnp.int32)
    slots = jnp.sum(jnp.cumsum(marks, axis=0) * marks, axis=1) - 1
    places = chosen * capacity + slots
    owners = jnp.arange(chosen.shape[0], dtype=jnp.int32) // top_count
    table = jnp.zeros((experts * capacity,), jnp.int32).at[places].set(owners)
    filled = jnp.zeros((experts * capacity,), jnp.bool_).at[places].set(True)
    outbound = jnp.where(filled[:, None], normed[table], jnp.zeros((), jnp.bfloat16))
    outbound = outbound.reshape(experts, capacity, width)
    arrived = lax.all_to_all(outbound, "ep", split_axis=0, concat_axis=0, tiled=True).reshape(
        experts * capacity, width
    )
    hidden = swiglu_rows(arrived, expert_gate[0], expert_up[0])
    results = jnp.dot(
        hidden,
        lax.all_gather(expert_down[0], "tp", axis=1, tiled=True),
        preferred_element_type=jnp.float32,
    ).astype(jnp.bfloat16)
    returned = lax.all_to_all(
        results.reshape(experts, capacity, width), "ep", split_axis=0, concat_axis=0, tiled=True
    )
    returned = returned.reshape(experts * capacity, width)
    picked = returned[places].astype(jnp.float32).reshape(count_tokens, top_count, width)
    routed = jnp.sum(picked * route_weights[:, :, None], axis=1)
    shared_hidden = swiglu_rows(normed, shared_gate, shared_up)
    shared_out = jnp.dot(
        shared_hidden,
        lax.all_gather(shared_down, "tp", axis=1, tiled=True),
        preferred_element_type=jnp.float32,
    )
    moe = (shared_out + routed).astype(jnp.bfloat16)
    columns = lax.all_to_all(moe, "tp", split_axis=1, concat_axis=0, tiled=True)
    values = columns.astype(jnp.float32)
    own_rows = moe.astype(jnp.float32)
    totals = lax.all_gather(jnp.sum(own_rows * own_rows, axis=1), "tp", axis=0, tiled=True)
    scale = lax.rsqrt(totals / width + 1e-06)
    return (values * scale[:, None] * out_gain[None, :]).astype(jnp.bfloat16)


def per_device(tokens, routes, *rest):
    count, width = tokens.shape
    experts, blocks = lax.axis_size("ep"), lax.axis_size("tp")
    capacity = 3 * count * routes.shape[1] // (2 * experts)
    powers = experts & (experts - 1) == 0 and blocks & (blocks - 1) == 0
    aligned = capacity % 16 == 0 and width // blocks % 128 == 0 and count % 128 == 0
    fits = powers and aligned and experts >= 8
    return (fast_device if fits else plain_device)(tokens, routes, *rest)


def solution(mesh):
    in_specs = (
        P(("ep", "tp"), None),
        P(("ep", "tp"), None),
        P(("ep", "tp"), None),
        P(),
        P("ep", None, None),
        P("ep", None, None),
        P("ep", None, "tp"),
        P(),
        P(),
        P(None, "tp"),
        P("tp"),
    )
    out_specs = P("ep", "tp")
    return jax.shard_map(
        per_device, mesh=mesh, in_specs=in_specs, out_specs=out_specs, check_vma=False
    )
```

```python
import functools

import jax
import jax.numpy as jnp
from jax import lax
from jax.experimental import pallas as pl
from jax.experimental.pallas import tpu as pltpu
from jax.sharding import PartitionSpec as P


VMEM = pl.BlockSpec(memory_space=pltpu.VMEM)
SMEM = pl.BlockSpec(memory_space=pltpu.SMEM)
HBM = pl.BlockSpec(memory_space=pltpu.HBM)
F32 = jnp.float32
BF16 = jnp.bfloat16


def dot(a, b):
    return jnp.dot(a, b, preferred_element_type=F32)


def call(kernel, outs, inputs, flops, scalars=0, far=(), scratch=(), far_out=False):
    moved = sum(a.size * a.dtype.itemsize for a in inputs)
    moved += sum(o.size * o.dtype.itemsize for o in outs)
    specs = [SMEM] * scalars + [VMEM] * (len(inputs) - scalars)
    for i in far:
        specs[i] = HBM
        inputs[i] = pltpu.with_memory_space_constraint(inputs[i], pltpu.HBM)
    return pl.pallas_call(
        kernel,
        out_shape=outs,
        in_specs=specs,
        out_specs=[HBM if far_out else VMEM] * len(outs),
        scratch_shapes=scratch,
        cost_estimate=pl.CostEstimate(flops=flops, bytes_accessed=moved, transcendentals=0),
        compiler_params=pltpu.CompilerParams(vmem_limit_bytes=40 * 1024 * 1024),
    )(*inputs)


def fetch(sources, targets, sems):
    copies = [
        pltpu.make_async_copy(source, target, sems.at[i])
        for i, (source, target) in enumerate(zip(sources, targets))
    ]
    for copy in copies:
        copy.start()
    return copies


def swiglu(rows, both):
    parts = dot(rows, both)
    inner = parts.shape[1] // 2
    gate_part, up_part = parts[:, :inner], parts[:, inner:]
    return (gate_part / (1.0 + jnp.exp(-gate_part)) * up_part).astype(BF16)


def normalize(values, gain):
    values = values.astype(F32)
    inverse = lax.rsqrt(jnp.mean(values * values, axis=1, keepdims=True) + 1e-06)
    return (values * inverse * gain).astype(BF16)


def prepare_kernel(experts, capacity, me, *refs):
    pieces = refs[2 : 2 + experts]
    tokens, routes, sems = refs[2 + experts :]
    copies = fetch(refs[:2], (tokens, routes), sems)
    copies[1].wait()
    count = tokens.shape[0]
    index = lax.broadcasted_iota(jnp.int32, (experts, count), 0)
    marks = [index == routes[j : j + 1, :] for j in range(routes.shape[0])]
    marked = functools.reduce(jnp.logical_or, marks)
    earlier = lax.broadcasted_iota(jnp.int32, (count, count), 0) < lax.broadcasted_iota(
        jnp.int32, (count, count), 1
    )
    before = dot(marked.astype(BF16), earlier.astype(BF16))
    places = []
    for j, mark in enumerate(marks):
        slot = jnp.sum(jnp.where(mark, before, 0.0), axis=0, keepdims=True)
        places.append((routes[j : j + 1, :] ^ me[0]) * capacity + slot.astype(jnp.int32))
    copies[0].wait()
    rows = tokens[...]
    half = experts // 2
    for start in (half, 0):
        at = lax.broadcasted_iota(jnp.int32, (half * capacity, count), 0) + start * capacity
        chosen = functools.reduce(jnp.logical_or, [at == place for place in places])
        moved = dot(chosen.astype(F32).astype(BF16), rows).astype(BF16)
        for k in range(half):
            pieces[start + k][...] = moved[k * capacity : (k + 1) * capacity]


def table_kernel(capacity, groups, me, *refs):
    packed, outs = refs[: -len(groups)], refs[-len(groups) :]
    for m, ref in enumerate(packed):
        top_count = ref.shape[0] // 2
        count = ref.shape[1]
        columns = [
            jnp.broadcast_to(ref[r : r + 1, :], (count, count)).T for r in range(2 * top_count)
        ]
        lane = lax.broadcasted_iota(jnp.int32, (count, count), 1)
        chosen = [c.astype(jnp.int32) for c in columns[:top_count]]
        marks = [lane == c for c in chosen]
        marked = functools.reduce(jnp.logical_or, marks)
        earlier = lax.broadcasted_iota(jnp.int32, (count, count), 0) > lane
        before = dot(earlier.astype(F32).astype(BF16), marked.astype(F32).astype(BF16))
        places = []
        for c, mark in zip(chosen, marks):
            slot = jnp.sum(jnp.where(mark, before, 0.0), axis=1, keepdims=True)
            places.append((c[:, :1] ^ me[0]) * capacity + slot.astype(jnp.int32))
        for (start, size), out in zip(groups, outs):
            wide = size * capacity
            at = lax.broadcasted_iota(jnp.int32, (count, wide), 1) + start * capacity
            table = functools.reduce(
                jnp.add,
                [
                    jnp.where(at == place, weight[:, :1], 0.0)
                    for place, weight in zip(places, columns[top_count:])
                ],
            )
            parts = []
            for _ in range(3):
                piece = table.astype(BF16)
                parts.append(piece)
                table = table - piece.astype(F32)
            out[m] = jnp.concatenate(parts, axis=1)


def stage_kernel(gate, upward, held, both, sems):
    inner = gate.shape[1]
    for copy in fetch((gate, upward), (both.at[:, :inner], both.at[:, inner:]), sems):
        copy.wait()


def shared_kernel(tokens, gain, gate, upward, hidden, both, sems):
    inner = gate.shape[1]
    copies = fetch((gate, upward), (both.at[:, :inner], both.at[:, inner:]), sems)
    rows = normalize(tokens[...], gain[...])
    for copy in copies:
        copy.wait()
    hidden[...] = swiglu(rows, both[...])


def hidden_kernel(*refs):
    gain, both, out = refs[-3:]
    rows = jnp.concatenate([r[...] for r in refs[:-3]], axis=0)
    out[...] = swiglu(normalize(rows, gain[...]), both[...])


def down_kernel(blocks, units, capacity, *refs):
    hidden = refs[:blocks]
    down = refs[blocks]
    outs = refs[blocks + 1 :]
    count = units * capacity
    rows = jnp.concatenate([h[...] for h in hidden], axis=0)
    result = dot(rows, down[...]).astype(BF16)
    for u in range(units):
        for m in range(blocks):
            first = m * count + u * capacity
            outs[u][m] = result[first : first + capacity]


def weighted(table, returned, m):
    rows = jnp.concatenate([r[m] for r in returned], axis=0)
    return dot(table[m], jnp.concatenate([rows] * 3, axis=0))


def base_kernel(blocks, *refs):
    hidden = refs[:blocks]
    down, table = refs[blocks : blocks + 2]
    returned, out = refs[blocks + 2 : -1], refs[-1]
    shared = dot(jnp.concatenate([h[...] for h in hidden], axis=0), down[...])
    count = out.shape[1]
    for m in range(blocks):
        out[m] = shared[m * count : (m + 1) * count] + weighted(table, returned, m)


def more_kernel(blocks, total, table, *refs):
    for m in range(blocks):
        refs[-1][m] = total[m] + weighted(table, refs[:-1], m)


def finish_kernel(blocks, lanes, total, table, *refs):
    returned = refs[:-2]
    moe, squares = refs[-2:]
    ones = jnp.ones((8, lanes), F32)
    for m in range(blocks):
        rounded = (total[m] + weighted(table, returned, m)).astype(BF16)
        moe[m] = rounded
        wide = rounded.astype(F32)
        wide = wide * wide
        folded = functools.reduce(
            jnp.add,
            [wide[:, at : at + lanes] for at in range(0, wide.shape[1], lanes)],
        )
        sums = lax.dot_general(
            ones,
            folded,
            (((1,), (1,)), ((), ())),
            precision=lax.Precision.HIGHEST,
            preferred_element_type=F32,
        )
        squares[m : m + 1, :] = sums[:1]


def scale_kernel(blocks, width, me, moe, gain, *refs):
    squares, out, ready, sems = refs[:blocks], *refs[blocks:]
    count = moe.shape[1]
    copies = []
    for m in range(blocks):
        total = squares[0][m : m + 1, :]
        for p in range(1, blocks):
            total = total + squares[p][m ^ p : (m ^ p) + 1, :]
        scale = lax.rsqrt(total / width + 1e-06)
        column = jnp.broadcast_to(scale, (count, count)).T[:, :1]
        ready[m] = (moe[m].astype(F32) * column * gain[...]).astype(BF16)
        first = pl.multiple_of((me[0] ^ m) * count, count)
        copy = pltpu.make_async_copy(ready.at[m], out.at[pl.ds(first, count), :], sems.at[m])
        copy.start()
        copies.append(copy)
    for copy in copies:
        copy.wait()


def swap(array, axis, k):
    size = lax.axis_size(axis)
    return lax.ppermute(array, axis, [(s, s ^ k) for s in range(size)])


def spread(array):
    return [array] + [swap(array, "tp", m) for m in range(1, lax.axis_size("tp"))]


def fast_device(
    tokens,
    routes,
    route_weights,
    norm_gain,
    expert_gate,
    expert_up,
    expert_down,
    shared_gate,
    shared_up,
    shared_down,
    out_gain,
):
    count, width = tokens.shape
    top_count = routes.shape[1]
    experts = lax.axis_size("ep")
    blocks = lax.axis_size("tp")
    inner = expert_gate.shape[2]
    local = expert_down.shape[2]
    capacity = 3 * count * top_count // (2 * experts)
    row = lax.axis_index("ep").astype(jnp.int32).reshape(1)
    column = lax.axis_index("tp").astype(jnp.int32).reshape(1)
    piece = jax.ShapeDtypeStruct((capacity, width), BF16)
    gain = norm_gain[None, :]
    pieces = call(
        functools.partial(prepare_kernel, experts, capacity),
        [piece] * experts,
        [row, tokens, routes.T],
        2 * experts * capacity * count * width,
        scalars=1,
        far=(1, 2),
        scratch=[
            pltpu.VMEM((count, width), BF16),
            pltpu.VMEM((top_count, count), jnp.int32),
            pltpu.SemaphoreType.DMA((2,)),
        ],
    )
    half, quarter = experts // 2, experts // 4
    arrived = [pieces[0]] + [swap(pieces[k], "ep", k) for k in range(1, experts)]
    groups = {"N": (0, half), "A": (half, quarter), "B": (half + quarter, quarter)}

    packed = jnp.concatenate([routes.T.astype(F32), route_weights.T], axis=0)
    packed = spread(packed)
    both = jax.ShapeDtypeStruct((width, 2 * inner), BF16)
    (weights,) = call(
        stage_kernel,
        [both],
        [expert_gate[0], expert_up[0], pieces[0]],
        count * width,
        far=(0, 1, 2),
        scratch=[pltpu.SemaphoreType.DMA((2,))],
    )
    (shared,) = call(
        shared_kernel,
        [jax.ShapeDtypeStruct((count, inner), BF16)],
        [tokens, gain, shared_gate, shared_up],
        4 * count * width * inner,
        far=(2, 3),
        scratch=[pltpu.VMEM(both.shape, BF16), pltpu.SemaphoreType.DMA((2,))],
    )
    shared = spread(shared)
    tables = call(
        functools.partial(table_kernel, capacity, list(groups.values())),
        [
            jax.ShapeDtypeStruct((blocks, count, 3 * size * capacity), BF16)
            for _, size in groups.values()
        ],
        [row] + packed,
        blocks * count * count * count,
        scalars=1,
    )

    returned = {}
    for name, (first, size) in groups.items():
        rows = size * capacity
        (hidden,) = call(
            hidden_kernel,
            [jax.ShapeDtypeStruct((rows, inner), BF16)],
            arrived[first : first + size] + [gain, weights],
            4 * rows * width * inner,
        )
        results = call(
            functools.partial(down_kernel, blocks, size, capacity),
            [jax.ShapeDtypeStruct((blocks, capacity, local), BF16)] * size,
            spread(hidden) + [expert_down[0]],
            2 * blocks * rows * inner * local,
        )
        returned[name] = [
            swap(results[u], "ep", first + u) if first + u else results[u]
            for u in range(size)
        ]

    sums = jax.ShapeDtypeStruct((blocks, count, local), F32)
    (total,) = call(
        functools.partial(base_kernel, blocks),
        [sums],
        shared + [shared_down, tables[0]] + returned["N"],
        2 * blocks * count * local * (inner + 3 * half * capacity),
    )
    (total,) = call(
        functools.partial(more_kernel, blocks),
        [sums],
        [total, tables[1]] + returned["A"],
        2 * blocks * count * local * 3 * quarter * capacity,
    )
    moe, squares = call(
        functools.partial(finish_kernel, blocks, 128),
        [
            jax.ShapeDtypeStruct((blocks, count, local), BF16),
            jax.ShapeDtypeStruct((blocks, count), F32),
        ],
        [total, tables[2]] + returned["B"],
        2 * blocks * count * local * 3 * quarter * capacity,
    )
    (out,) = call(
        functools.partial(scale_kernel, blocks, width),
        [jax.ShapeDtypeStruct((blocks * count, local), BF16)],
        [column, moe, out_gain[None, :]] + spread(squares),
        4 * blocks * count * local,
        scalars=1,
        scratch=[
            pltpu.VMEM((blocks, count, local), BF16),
            pltpu.SemaphoreType.DMA((blocks,)),
        ],
        far_out=True,
    )
    return out


def swiglu_rows(rows, gate, upward):
    gate_part = jnp.dot(rows, gate, preferred_element_type=jnp.float32)
    up_part = jnp.dot(rows, upward, preferred_element_type=jnp.float32)
    return (jax.nn.silu(gate_part) * up_part).astype(jnp.bfloat16)


def plain_device(
    tokens,
    routes,
    route_weights,
    norm_gain,
    expert_gate,
    expert_up,
    expert_down,
    shared_gate,
    shared_up,
    shared_down,
    out_gain,
):
    count_tokens, width = tokens.shape
    top_count = routes.shape[1]
    experts = lax.axis_size("ep")
    capacity = max(2, 3 * count_tokens * top_count // (2 * experts))
    tokens_f32 = tokens.astype(jnp.float32)
    inverse = lax.rsqrt(jnp.mean(tokens_f32 * tokens_f32, axis=1, keepdims=True) + 1e-06)
    normed = (tokens_f32 * inverse * norm_gain[None, :]).astype(jnp.bfloat16)
    chosen = routes.reshape(-1)
    marks = (chosen[:, None] == jnp.arange(experts, dtype=jnp.int32)[None, :]).astype(jnp.int32)
    slots = jnp.sum(jnp.cumsum(marks, axis=0) * marks, axis=1) - 1
    places = chosen * capacity + slots
    owners = jnp.arange(chosen.shape[0], dtype=jnp.int32) // top_count
    table = jnp.zeros((experts * capacity,), jnp.int32).at[places].set(owners)
    filled = jnp.zeros((experts * capacity,), jnp.bool_).at[places].set(True)
    outbound = jnp.where(filled[:, None], normed[table], jnp.zeros((), jnp.bfloat16))
    outbound = outbound.reshape(experts, capacity, width)
    arrived = lax.all_to_all(outbound, "ep", split_axis=0, concat_axis=0, tiled=True).reshape(
        experts * capacity, width
    )
    hidden = swiglu_rows(arrived, expert_gate[0], expert_up[0])
    results = jnp.dot(
        hidden,
        lax.all_gather(expert_down[0], "tp", axis=1, tiled=True),
        preferred_element_type=jnp.float32,
    ).astype(jnp.bfloat16)
    returned = lax.all_to_all(
        results.reshape(experts, capacity, width), "ep", split_axis=0, concat_axis=0, tiled=True
    )
    returned = returned.reshape(experts * capacity, width)
    picked = returned[places].astype(jnp.float32).reshape(count_tokens, top_count, width)
    routed = jnp.sum(picked * route_weights[:, :, None], axis=1)
    shared_hidden = swiglu_rows(normed, shared_gate, shared_up)
    shared_out = jnp.dot(
        shared_hidden,
        lax.all_gather(shared_down, "tp", axis=1, tiled=True),
        preferred_element_type=jnp.float32,
    )
    moe = (shared_out + routed).astype(jnp.bfloat16)
    columns = lax.all_to_all(moe, "tp", split_axis=1, concat_axis=0, tiled=True)
    values = columns.astype(jnp.float32)
    own_rows = moe.astype(jnp.float32)
    totals = lax.all_gather(jnp.sum(own_rows * own_rows, axis=1), "tp", axis=0, tiled=True)
    scale = lax.rsqrt(totals / width + 1e-06)
    return (values * scale[:, None] * out_gain[None, :]).astype(jnp.bfloat16)


def per_device(tokens, routes, *rest):
    count, width = tokens.shape
    experts, blocks = lax.axis_size("ep"), lax.axis_size("tp")
    capacity = 3 * count * routes.shape[1] // (2 * experts)
    powers = experts & (experts - 1) == 0 and blocks & (blocks - 1) == 0
    aligned = capacity % 16 == 0 and width // blocks % 128 == 0 and count % 128 == 0
    fits = powers and aligned and experts >= 8
    return (fast_device if fits else plain_device)(tokens, routes, *rest)


def solution(mesh):
    in_specs = (
        P(("ep", "tp"), None),
        P(("ep", "tp"), None),
        P(("ep", "tp"), None),
        P(),
        P("ep", None, None),
        P("ep", None, None),
        P("ep", None, "tp"),
        P(),
        P(),
        P(None, "tp"),
        P("tp"),
    )
    out_specs = P("ep", "tp")
    return jax.shard_map(
        per_device, mesh=mesh, in_specs=in_specs, out_specs=out_specs, check_vma=False
    )
```

```python
import functools

import jax
import jax.numpy as jnp
from jax import lax
from jax.experimental import pallas as pl
from jax.experimental.pallas import tpu as pltpu
from jax.sharding import PartitionSpec as P


VMEM = pl.BlockSpec(memory_space=pltpu.VMEM)
SMEM = pl.BlockSpec(memory_space=pltpu.SMEM)
HBM = pl.BlockSpec(memory_space=pltpu.HBM)
F32 = jnp.float32
BF16 = jnp.bfloat16


def dot(a, b):
    return jnp.dot(a, b, preferred_element_type=F32)


def call(kernel, outs, inputs, flops, scalars=0, far=(), scratch=(), far_out=False):
    moved = sum(a.size * a.dtype.itemsize for a in inputs)
    moved += sum(o.size * o.dtype.itemsize for o in outs)
    specs = [SMEM] * scalars + [VMEM] * (len(inputs) - scalars)
    for i in far:
        specs[i] = HBM
        inputs[i] = pltpu.with_memory_space_constraint(inputs[i], pltpu.HBM)
    return pl.pallas_call(
        kernel,
        out_shape=outs,
        in_specs=specs,
        out_specs=[HBM if far_out else VMEM] * len(outs),
        scratch_shapes=scratch,
        cost_estimate=pl.CostEstimate(flops=flops, bytes_accessed=moved, transcendentals=0),
        compiler_params=pltpu.CompilerParams(vmem_limit_bytes=40 * 1024 * 1024),
    )(*inputs)


def fetch(sources, targets, sems):
    copies = [
        pltpu.make_async_copy(source, target, sems.at[i])
        for i, (source, target) in enumerate(zip(sources, targets))
    ]
    for copy in copies:
        copy.start()
    return copies


def swiglu(rows, both):
    parts = dot(rows, both)
    inner = parts.shape[1] // 2
    gate_part, up_part = parts[:, :inner], parts[:, inner:]
    return (gate_part / (1.0 + jnp.exp(-gate_part)) * up_part).astype(BF16)


def normalize(values, gain):
    values = values.astype(F32)
    inverse = lax.rsqrt(jnp.mean(values * values, axis=1, keepdims=True) + 1e-06)
    return (values * inverse * gain).astype(BF16)


def prepare_kernel(experts, capacity, me, *refs):
    pieces = refs[2 : 2 + experts]
    tokens, routes, sems = refs[2 + experts :]
    copies = fetch(refs[:2], (tokens, routes), sems)
    copies[1].wait()
    count = tokens.shape[0]
    index = lax.broadcasted_iota(jnp.int32, (experts, count), 0)
    marks = [index == routes[j : j + 1, :] for j in range(routes.shape[0])]
    marked = functools.reduce(jnp.logical_or, marks)
    earlier = lax.broadcasted_iota(jnp.int32, (count, count), 0) < lax.broadcasted_iota(
        jnp.int32, (count, count), 1
    )
    before = dot(marked.astype(BF16), earlier.astype(BF16))
    places = []
    for j, mark in enumerate(marks):
        slot = jnp.sum(jnp.where(mark, before, 0.0), axis=0, keepdims=True)
        places.append((routes[j : j + 1, :] ^ me[0]) * capacity + slot.astype(jnp.int32))
    copies[0].wait()
    rows = tokens[...]
    half = experts // 2
    for start in (half, 0):
        at = lax.broadcasted_iota(jnp.int32, (half * capacity, count), 0) + start * capacity
        chosen = functools.reduce(jnp.logical_or, [at == place for place in places])
        moved = dot(chosen.astype(F32).astype(BF16), rows).astype(BF16)
        for k in range(half):
            pieces[start + k][...] = moved[k * capacity : (k + 1) * capacity]


def table_kernel(capacity, groups, me, *refs):
    packed, outs = refs[: -len(groups)], refs[-len(groups) :]
    for m, ref in enumerate(packed):
        top_count = ref.shape[0] // 2
        count = ref.shape[1]
        columns = [
            jnp.broadcast_to(ref[r : r + 1, :], (count, count)).T for r in range(2 * top_count)
        ]
        lane = lax.broadcasted_iota(jnp.int32, (count, count), 1)
        chosen = [c.astype(jnp.int32) for c in columns[:top_count]]
        marks = [lane == c for c in chosen]
        marked = functools.reduce(jnp.logical_or, marks)
        earlier = lax.broadcasted_iota(jnp.int32, (count, count), 0) > lane
        before = dot(earlier.astype(F32).astype(BF16), marked.astype(F32).astype(BF16))
        places = []
        for c, mark in zip(chosen, marks):
            slot = jnp.sum(jnp.where(mark, before, 0.0), axis=1, keepdims=True)
            places.append((c[:, :1] ^ me[0]) * capacity + slot.astype(jnp.int32))
        for (start, size), out in zip(groups, outs):
            wide = size * capacity
            at = lax.broadcasted_iota(jnp.int32, (count, wide), 1) + start * capacity
            table = functools.reduce(
                jnp.add,
                [
                    jnp.where(at == place, weight[:, :1], 0.0)
                    for place, weight in zip(places, columns[top_count:])
                ],
            )
            parts = []
            for _ in range(3):
                piece = table.astype(BF16)
                parts.append(piece)
                table = table - piece.astype(F32)
            out[m] = jnp.concatenate(parts, axis=1)


def stage_kernel(gate, upward, held, both, sems):
    inner = gate.shape[1]
    for copy in fetch((gate, upward), (both.at[:, :inner], both.at[:, inner:]), sems):
        copy.wait()


def shared_kernel(tokens, gain, gate, upward, hidden, both, sems):
    inner = gate.shape[1]
    copies = fetch((gate, upward), (both.at[:, :inner], both.at[:, inner:]), sems)
    rows = normalize(tokens[...], gain[...])
    for copy in copies:
        copy.wait()
    hidden[...] = swiglu(rows, both[...])


def hidden_kernel(*refs):
    gain, both, out = refs[-3:]
    rows = jnp.concatenate([r[...] for r in refs[:-3]], axis=0)
    out[...] = swiglu(normalize(rows, gain[...]), both[...])


def down_kernel(blocks, units, capacity, *refs):
    hidden = refs[:blocks]
    down = refs[blocks]
    outs = refs[blocks + 1 :]
    count = units * capacity
    rows = jnp.concatenate([h[...] for h in hidden], axis=0)
    result = dot(rows, down[...]).astype(BF16)
    for u in range(units):
        for m in range(blocks):
            first = m * count + u * capacity
            outs[u][m] = result[first : first + capacity]


def weighted(table, returned, m):
    rows = jnp.concatenate([r[m] for r in returned], axis=0)
    return dot(table[m], jnp.concatenate([rows] * 3, axis=0))


def base_kernel(blocks, *refs):
    hidden = refs[:blocks]
    down, table = refs[blocks : blocks + 2]
    returned, out = refs[blocks + 2 : -1], refs[-1]
    shared = dot(jnp.concatenate([h[...] for h in hidden], axis=0), down[...])
    count = out.shape[1]
    for m in range(blocks):
        out[m] = shared[m * count : (m + 1) * count] + weighted(table, returned, m)


def more_kernel(blocks, total, table, *refs):
    for m in range(blocks):
        refs[-1][m] = total[m] + weighted(table, refs[:-1], m)


def finish_kernel(blocks, total, table, *refs):
    returned = refs[:-2]
    moe, squares = refs[-2:]
    count = moe.shape[1]
    lane = lax.broadcasted_iota(jnp.int32, (count, count), 1)
    sums = jnp.zeros((count, count), F32)
    for m in range(blocks):
        rounded = (total[m] + weighted(table, returned, m)).astype(BF16)
        moe[m] = rounded
        wide = rounded.astype(F32)
        sums = jnp.where(lane == m, jnp.sum(wide * wide, axis=1, keepdims=True), sums)
    squares[...] = sums.T[:blocks, :]


def scale_kernel(blocks, width, me, moe, gain, *refs):
    squares, out, ready, sems = refs[:blocks], *refs[blocks:]
    count = moe.shape[1]
    totals = []
    for m in range(blocks):
        total = squares[0][m : m + 1, :]
        for p in range(1, blocks):
            total = total + squares[p][m ^ p : (m ^ p) + 1, :]
        totals.append(lax.rsqrt(total / width + 1e-06))
    totals.append(jnp.zeros((count - blocks, count), F32))
    columns = jnp.concatenate(totals, axis=0).T
    copies = []
    for m in range(blocks):
        column = columns[:, m : m + 1]
        ready[m] = (moe[m].astype(F32) * column * gain[...]).astype(BF16)
        first = pl.multiple_of((me[0] ^ m) * count, count)
        copy = pltpu.make_async_copy(ready.at[m], out.at[pl.ds(first, count), :], sems.at[m])
        copy.start()
        copies.append(copy)
    for copy in copies:
        copy.wait()


def swap(array, axis, k):
    size = lax.axis_size(axis)
    return lax.ppermute(array, axis, [(s, s ^ k) for s in range(size)])


def spread(array):
    return [array] + [swap(array, "tp", m) for m in range(1, lax.axis_size("tp"))]


def fast_device(
    tokens,
    routes,
    route_weights,
    norm_gain,
    expert_gate,
    expert_up,
    expert_down,
    shared_gate,
    shared_up,
    shared_down,
    out_gain,
):
    count, width = tokens.shape
    top_count = routes.shape[1]
    experts = lax.axis_size("ep")
    blocks = lax.axis_size("tp")
    inner = expert_gate.shape[2]
    local = expert_down.shape[2]
    capacity = 3 * count * top_count // (2 * experts)
    row = lax.axis_index("ep").astype(jnp.int32).reshape(1)
    column = lax.axis_index("tp").astype(jnp.int32).reshape(1)
    piece = jax.ShapeDtypeStruct((capacity, width), BF16)
    gain = norm_gain[None, :]
    pieces = call(
        functools.partial(prepare_kernel, experts, capacity),
        [piece] * experts,
        [row, tokens, routes.T],
        2 * experts * capacity * count * width,
        scalars=1,
        far=(1, 2),
        scratch=[
            pltpu.VMEM((count, width), BF16),
            pltpu.VMEM((top_count, count), jnp.int32),
            pltpu.SemaphoreType.DMA((2,)),
        ],
    )
    half, quarter = experts // 2, experts // 4
    arrived = [pieces[0]] + [swap(pieces[k], "ep", k) for k in range(1, experts)]
    groups = {"N": (0, half), "A": (half, quarter), "B": (half + quarter, quarter)}

    packed = jnp.concatenate([routes.T.astype(F32), route_weights.T], axis=0)
    packed = spread(packed)
    both = jax.ShapeDtypeStruct((width, 2 * inner), BF16)
    (weights,) = call(
        stage_kernel,
        [both],
        [expert_gate[0], expert_up[0], pieces[0]],
        count * width,
        far=(0, 1),
        scratch=[pltpu.SemaphoreType.DMA((2,))],
    )
    (shared,) = call(
        shared_kernel,
        [jax.ShapeDtypeStruct((count, inner), BF16)],
        [tokens, gain, shared_gate, shared_up],
        4 * count * width * inner,
        far=(2, 3),
        scratch=[pltpu.VMEM(both.shape, BF16), pltpu.SemaphoreType.DMA((2,))],
    )
    shared = spread(shared)
    tables = call(
        functools.partial(table_kernel, capacity, list(groups.values())),
        [
            jax.ShapeDtypeStruct((blocks, count, 3 * size * capacity), BF16)
            for _, size in groups.values()
        ],
        [row] + packed,
        blocks * count * count * count,
        scalars=1,
    )

    returned = {}
    for name, (first, size) in groups.items():
        rows = size * capacity
        (hidden,) = call(
            hidden_kernel,
            [jax.ShapeDtypeStruct((rows, inner), BF16)],
            arrived[first : first + size] + [gain, weights],
            4 * rows * width * inner,
        )
        results = call(
            functools.partial(down_kernel, blocks, size, capacity),
            [jax.ShapeDtypeStruct((blocks, capacity, local), BF16)] * size,
            spread(hidden) + [expert_down[0]],
            2 * blocks * rows * inner * local,
        )
        returned[name] = [
            swap(results[u], "ep", first + u) if first + u else results[u]
            for u in range(size)
        ]

    sums = jax.ShapeDtypeStruct((blocks, count, local), F32)
    (total,) = call(
        functools.partial(base_kernel, blocks),
        [sums],
        shared + [shared_down, tables[0]] + returned["N"],
        2 * blocks * count * local * (inner + 3 * half * capacity),
    )
    (total,) = call(
        functools.partial(more_kernel, blocks),
        [sums],
        [total, tables[1]] + returned["A"],
        2 * blocks * count * local * 3 * quarter * capacity,
    )
    moe, squares = call(
        functools.partial(finish_kernel, blocks),
        [
            jax.ShapeDtypeStruct((blocks, count, local), BF16),
            jax.ShapeDtypeStruct((blocks, count), F32),
        ],
        [total, tables[2]] + returned["B"],
        2 * blocks * count * local * 3 * quarter * capacity,
    )
    (out,) = call(
        functools.partial(scale_kernel, blocks, width),
        [jax.ShapeDtypeStruct((blocks * count, local), BF16)],
        [column, moe, out_gain[None, :]] + spread(squares),
        4 * blocks * count * local,
        scalars=1,
        scratch=[
            pltpu.VMEM((blocks, count, local), BF16),
            pltpu.SemaphoreType.DMA((blocks,)),
        ],
        far_out=True,
    )
    return out


def swiglu_rows(rows, gate, upward):
    gate_part = jnp.dot(rows, gate, preferred_element_type=jnp.float32)
    up_part = jnp.dot(rows, upward, preferred_element_type=jnp.float32)
    return (jax.nn.silu(gate_part) * up_part).astype(jnp.bfloat16)


def plain_device(
    tokens,
    routes,
    route_weights,
    norm_gain,
    expert_gate,
    expert_up,
    expert_down,
    shared_gate,
    shared_up,
    shared_down,
    out_gain,
):
    count_tokens, width = tokens.shape
    top_count = routes.shape[1]
    experts = lax.axis_size("ep")
    capacity = max(2, 3 * count_tokens * top_count // (2 * experts))
    tokens_f32 = tokens.astype(jnp.float32)
    inverse = lax.rsqrt(jnp.mean(tokens_f32 * tokens_f32, axis=1, keepdims=True) + 1e-06)
    normed = (tokens_f32 * inverse * norm_gain[None, :]).astype(jnp.bfloat16)
    chosen = routes.reshape(-1)
    marks = (chosen[:, None] == jnp.arange(experts, dtype=jnp.int32)[None, :]).astype(jnp.int32)
    slots = jnp.sum(jnp.cumsum(marks, axis=0) * marks, axis=1) - 1
    places = chosen * capacity + slots
    owners = jnp.arange(chosen.shape[0], dtype=jnp.int32) // top_count
    table = jnp.zeros((experts * capacity,), jnp.int32).at[places].set(owners)
    filled = jnp.zeros((experts * capacity,), jnp.bool_).at[places].set(True)
    outbound = jnp.where(filled[:, None], normed[table], jnp.zeros((), jnp.bfloat16))
    outbound = outbound.reshape(experts, capacity, width)
    arrived = lax.all_to_all(outbound, "ep", split_axis=0, concat_axis=0, tiled=True).reshape(
        experts * capacity, width
    )
    hidden = swiglu_rows(arrived, expert_gate[0], expert_up[0])
    results = jnp.dot(
        hidden,
        lax.all_gather(expert_down[0], "tp", axis=1, tiled=True),
        preferred_element_type=jnp.float32,
    ).astype(jnp.bfloat16)
    returned = lax.all_to_all(
        results.reshape(experts, capacity, width), "ep", split_axis=0, concat_axis=0, tiled=True
    )
    returned = returned.reshape(experts * capacity, width)
    picked = returned[places].astype(jnp.float32).reshape(count_tokens, top_count, width)
    routed = jnp.sum(picked * route_weights[:, :, None], axis=1)
    shared_hidden = swiglu_rows(normed, shared_gate, shared_up)
    shared_out = jnp.dot(
        shared_hidden,
        lax.all_gather(shared_down, "tp", axis=1, tiled=True),
        preferred_element_type=jnp.float32,
    )
    moe = (shared_out + routed).astype(jnp.bfloat16)
    columns = lax.all_to_all(moe, "tp", split_axis=1, concat_axis=0, tiled=True)
    values = columns.astype(jnp.float32)
    own_rows = moe.astype(jnp.float32)
    totals = lax.all_gather(jnp.sum(own_rows * own_rows, axis=1), "tp", axis=0, tiled=True)
    scale = lax.rsqrt(totals / width + 1e-06)
    return (values * scale[:, None] * out_gain[None, :]).astype(jnp.bfloat16)


def per_device(tokens, routes, *rest):
    count, width = tokens.shape
    experts, blocks = lax.axis_size("ep"), lax.axis_size("tp")
    capacity = 3 * count * routes.shape[1] // (2 * experts)
    powers = experts & (experts - 1) == 0 and blocks & (blocks - 1) == 0
    aligned = capacity % 16 == 0 and width // blocks % 128 == 0 and count % 128 == 0
    fits = powers and aligned and experts >= 8
    return (fast_device if fits else plain_device)(tokens, routes, *rest)


def solution(mesh):
    in_specs = (
        P(("ep", "tp"), None),
        P(("ep", "tp"), None),
        P(("ep", "tp"), None),
        P(),
        P("ep", None, None),
        P("ep", None, None),
        P("ep", None, "tp"),
        P(),
        P(),
        P(None, "tp"),
        P("tp"),
    )
    out_specs = P("ep", "tp")
    return jax.shard_map(
        per_device, mesh=mesh, in_specs=in_specs, out_specs=out_specs, check_vma=False
    )
```

```python
import functools

import jax
import jax.numpy as jnp
from jax import lax
from jax.experimental import pallas as pl
from jax.experimental.pallas import tpu as pltpu
from jax.sharding import PartitionSpec as P


VMEM = pl.BlockSpec(memory_space=pltpu.VMEM)
SMEM = pl.BlockSpec(memory_space=pltpu.SMEM)
HBM = pl.BlockSpec(memory_space=pltpu.HBM)
F32 = jnp.float32
BF16 = jnp.bfloat16


def dot(a, b):
    return jnp.dot(a, b, preferred_element_type=F32)


def call(kernel, outs, inputs, flops, scalars=0, far=(), scratch=(), far_out=False):
    moved = sum(a.size * a.dtype.itemsize for a in inputs)
    moved += sum(o.size * o.dtype.itemsize for o in outs)
    specs = [SMEM] * scalars + [VMEM] * (len(inputs) - scalars)
    for i in far:
        specs[i] = HBM
        inputs[i] = pltpu.with_memory_space_constraint(inputs[i], pltpu.HBM)
    return pl.pallas_call(
        kernel,
        out_shape=outs,
        in_specs=specs,
        out_specs=[HBM if far_out else VMEM] * len(outs),
        scratch_shapes=scratch,
        cost_estimate=pl.CostEstimate(flops=flops, bytes_accessed=moved, transcendentals=0),
        compiler_params=pltpu.CompilerParams(vmem_limit_bytes=40 * 1024 * 1024),
    )(*inputs)


def fetch(sources, targets, sems):
    copies = [
        pltpu.make_async_copy(source, target, sems.at[i])
        for i, (source, target) in enumerate(zip(sources, targets))
    ]
    for copy in copies:
        copy.start()
    return copies


def swiglu(rows, both):
    parts = dot(rows, both)
    inner = parts.shape[1] // 2
    gate_part, up_part = parts[:, :inner], parts[:, inner:]
    return (gate_part / (1.0 + jnp.exp(-gate_part)) * up_part).astype(BF16)


def normalize(values, gain):
    values = values.astype(F32)
    inverse = lax.rsqrt(jnp.mean(values * values, axis=1, keepdims=True) + 1e-06)
    return (values * inverse * gain).astype(BF16)


def prepare_kernel(experts, capacity, me, *refs):
    pieces = refs[2 : 2 + experts]
    tokens, routes, sems = refs[2 + experts :]
    copies = fetch(refs[:2], (tokens, routes), sems)
    copies[1].wait()
    count = tokens.shape[0]
    index = lax.broadcasted_iota(jnp.int32, (experts, count), 0)
    marks = [index == routes[j : j + 1, :] for j in range(routes.shape[0])]
    marked = functools.reduce(jnp.logical_or, marks)
    earlier = lax.broadcasted_iota(jnp.int32, (count, count), 0) < lax.broadcasted_iota(
        jnp.int32, (count, count), 1
    )
    before = dot(marked.astype(BF16), earlier.astype(BF16))
    places = []
    for j, mark in enumerate(marks):
        slot = jnp.sum(jnp.where(mark, before, 0.0), axis=0, keepdims=True)
        places.append((routes[j : j + 1, :] ^ me[0]) * capacity + slot.astype(jnp.int32))
    copies[0].wait()
    rows = tokens[...]
    half = experts // 2
    for start in (half, 0):
        at = lax.broadcasted_iota(jnp.int32, (half * capacity, count), 0) + start * capacity
        chosen = functools.reduce(jnp.logical_or, [at == place for place in places])
        moved = dot(chosen.astype(F32).astype(BF16), rows).astype(BF16)
        for k in range(half):
            pieces[start + k][...] = moved[k * capacity : (k + 1) * capacity]


def table_kernel(capacity, groups, me, *refs):
    packed, outs = refs[: -len(groups)], refs[-len(groups) :]
    for m, ref in enumerate(packed):
        top_count = ref.shape[0] // 2
        count = ref.shape[1]
        columns = [
            jnp.broadcast_to(ref[r : r + 1, :], (count, count)).T for r in range(2 * top_count)
        ]
        lane = lax.broadcasted_iota(jnp.int32, (count, count), 1)
        chosen = [c.astype(jnp.int32) for c in columns[:top_count]]
        marks = [lane == c for c in chosen]
        marked = functools.reduce(jnp.logical_or, marks)
        earlier = lax.broadcasted_iota(jnp.int32, (count, count), 0) > lane
        before = dot(earlier.astype(F32).astype(BF16), marked.astype(F32).astype(BF16))
        places = []
        for c, mark in zip(chosen, marks):
            slot = jnp.sum(jnp.where(mark, before, 0.0), axis=1, keepdims=True)
            places.append((c[:, :1] ^ me[0]) * capacity + slot.astype(jnp.int32))
        for (start, size), out in zip(groups, outs):
            wide = size * capacity
            at = lax.broadcasted_iota(jnp.int32, (count, wide), 1) + start * capacity
            table = functools.reduce(
                jnp.add,
                [
                    jnp.where(at == place, weight[:, :1], 0.0)
                    for place, weight in zip(places, columns[top_count:])
                ],
            )
            parts = []
            for _ in range(3):
                piece = table.astype(BF16)
                parts.append(piece)
                table = table - piece.astype(F32)
            out[m] = jnp.concatenate(parts, axis=1)


def stage_kernel(gate, upward, held, both, sems):
    inner = gate.shape[1]
    for copy in fetch((gate, upward), (both.at[:, :inner], both.at[:, inner:]), sems):
        copy.wait()


def shared_kernel(tokens, gain, gate, upward, hidden, both, sems):
    inner = gate.shape[1]
    copies = fetch((gate, upward), (both.at[:, :inner], both.at[:, inner:]), sems)
    rows = normalize(tokens[...], gain[...])
    for copy in copies:
        copy.wait()
    hidden[...] = swiglu(rows, both[...])


def hidden_kernel(*refs):
    gain, both, out = refs[-3:]
    rows = jnp.concatenate([r[...] for r in refs[:-3]], axis=0)
    out[...] = swiglu(normalize(rows, gain[...]), both[...])


def down_kernel(blocks, units, capacity, *refs):
    hidden = refs[:blocks]
    down = refs[blocks]
    outs = refs[blocks + 1 :]
    count = units * capacity
    rows = jnp.concatenate([h[...] for h in hidden], axis=0)
    result = dot(rows, down[...]).astype(BF16)
    for u in range(units):
        for m in range(blocks):
            first = m * count + u * capacity
            outs[u][m] = result[first : first + capacity]


def weighted(table, returned, m):
    rows = jnp.concatenate([r[m] for r in returned], axis=0)
    return dot(table[m], jnp.concatenate([rows] * 3, axis=0))


def base_kernel(blocks, *refs):
    hidden = refs[:blocks]
    down, table = refs[blocks : blocks + 2]
    returned, out = refs[blocks + 2 : -1], refs[-1]
    shared = dot(jnp.concatenate([h[...] for h in hidden], axis=0), down[...])
    count = out.shape[1]
    for m in range(blocks):
        out[m] = shared[m * count : (m + 1) * count] + weighted(table, returned, m)


def more_kernel(blocks, total, table, *refs):
    for m in range(blocks):
        refs[-1][m] = total[m] + weighted(table, refs[:-1], m)


def finish_kernel(blocks, total, table, *refs):
    returned = refs[:-2]
    moe, squares = refs[-2:]
    count = moe.shape[1]
    lane = lax.broadcasted_iota(jnp.int32, (count, count), 1)
    sums = jnp.zeros((count, count), F32)
    for m in range(blocks):
        rounded = (total[m] + weighted(table, returned, m)).astype(BF16)
        moe[m] = rounded
        wide = rounded.astype(F32)
        sums = jnp.where(lane == m, jnp.sum(wide * wide, axis=1, keepdims=True), sums)
    squares[...] = sums.T[:blocks, :]


def scale_kernel(blocks, width, me, moe, gain, *refs):
    squares, out, ready, sems = refs[:blocks], *refs[blocks:]
    count = moe.shape[1]
    totals = []
    for m in range(blocks):
        total = squares[0][m : m + 1, :]
        for p in range(1, blocks):
            total = total + squares[p][m ^ p : (m ^ p) + 1, :]
        totals.append(lax.rsqrt(total / width + 1e-06))
    totals.append(jnp.zeros((count - blocks, count), F32))
    columns = jnp.concatenate(totals, axis=0).T
    copies = []
    for m in range(blocks):
        column = columns[:, m : m + 1]
        ready[m] = (moe[m].astype(F32) * column * gain[...]).astype(BF16)
        first = pl.multiple_of((me[0] ^ m) * count, count)
        copy = pltpu.make_async_copy(ready.at[m], out.at[pl.ds(first, count), :], sems.at[m])
        copy.start()
        copies.append(copy)
    for copy in copies:
        copy.wait()


def swap(array, axis, k):
    size = lax.axis_size(axis)
    return lax.ppermute(array, axis, [(s, s ^ k) for s in range(size)])


def spread(array):
    return [array] + [swap(array, "tp", m) for m in range(1, lax.axis_size("tp"))]


def fast_device(
    tokens,
    routes,
    route_weights,
    norm_gain,
    expert_gate,
    expert_up,
    expert_down,
    shared_gate,
    shared_up,
    shared_down,
    out_gain,
):
    count, width = tokens.shape
    top_count = routes.shape[1]
    experts = lax.axis_size("ep")
    blocks = lax.axis_size("tp")
    inner = expert_gate.shape[2]
    local = expert_down.shape[2]
    capacity = 3 * count * top_count // (2 * experts)
    row = lax.axis_index("ep").astype(jnp.int32).reshape(1)
    column = lax.axis_index("tp").astype(jnp.int32).reshape(1)
    piece = jax.ShapeDtypeStruct((capacity, width), BF16)
    gain = norm_gain[None, :]
    pieces = call(
        functools.partial(prepare_kernel, experts, capacity),
        [piece] * experts,
        [row, tokens, routes.T],
        2 * experts * capacity * count * width,
        scalars=1,
        far=(1, 2),
        scratch=[
            pltpu.VMEM((count, width), BF16),
            pltpu.VMEM((top_count, count), jnp.int32),
            pltpu.SemaphoreType.DMA((2,)),
        ],
    )
    half, quarter = experts // 2, experts // 4
    arrived = [pieces[0]] + [swap(pieces[k], "ep", k) for k in range(1, experts)]
    groups = {"N": (0, half), "A": (half + quarter, quarter), "B": (half, quarter)}

    packed = jnp.concatenate([routes.T.astype(F32), route_weights.T], axis=0)
    packed = spread(packed)
    both = jax.ShapeDtypeStruct((width, 2 * inner), BF16)
    (weights,) = call(
        stage_kernel,
        [both],
        [expert_gate[0], expert_up[0], pieces[0]],
        count * width,
        far=(0, 1),
        scratch=[pltpu.SemaphoreType.DMA((2,))],
    )
    (shared,) = call(
        shared_kernel,
        [jax.ShapeDtypeStruct((count, inner), BF16)],
        [tokens, gain, shared_gate, shared_up],
        4 * count * width * inner,
        far=(2, 3),
        scratch=[pltpu.VMEM(both.shape, BF16), pltpu.SemaphoreType.DMA((2,))],
    )
    shared = spread(shared)
    tables = call(
        functools.partial(table_kernel, capacity, list(groups.values())),
        [
            jax.ShapeDtypeStruct((blocks, count, 3 * size * capacity), BF16)
            for _, size in groups.values()
        ],
        [row] + packed,
        blocks * count * count * count,
        scalars=1,
    )

    returned = {}
    for name, (first, size) in groups.items():
        rows = size * capacity
        (hidden,) = call(
            hidden_kernel,
            [jax.ShapeDtypeStruct((rows, inner), BF16)],
            arrived[first : first + size] + [gain, weights],
            4 * rows * width * inner,
        )
        results = call(
            functools.partial(down_kernel, blocks, size, capacity),
            [jax.ShapeDtypeStruct((blocks, capacity, local), BF16)] * size,
            spread(hidden) + [expert_down[0]],
            2 * blocks * rows * inner * local,
        )
        returned[name] = [
            swap(results[u], "ep", first + u) if first + u else results[u]
            for u in range(size)
        ]

    sums = jax.ShapeDtypeStruct((blocks, count, local), F32)
    (total,) = call(
        functools.partial(base_kernel, blocks),
        [sums],
        shared + [shared_down, tables[1]] + returned["A"],
        2 * blocks * count * local * (inner + 3 * quarter * capacity),
    )
    (total,) = call(
        functools.partial(more_kernel, blocks),
        [sums],
        [total, tables[0]] + returned["N"],
        2 * blocks * count * local * 3 * half * capacity,
    )
    moe, squares = call(
        functools.partial(finish_kernel, blocks),
        [
            jax.ShapeDtypeStruct((blocks, count, local), BF16),
            jax.ShapeDtypeStruct((blocks, count), F32),
        ],
        [total, tables[2]] + returned["B"],
        2 * blocks * count * local * 3 * quarter * capacity,
    )
    (out,) = call(
        functools.partial(scale_kernel, blocks, width),
        [jax.ShapeDtypeStruct((blocks * count, local), BF16)],
        [column, moe, out_gain[None, :]] + spread(squares),
        4 * blocks * count * local,
        scalars=1,
        scratch=[
            pltpu.VMEM((blocks, count, local), BF16),
            pltpu.SemaphoreType.DMA((blocks,)),
        ],
        far_out=True,
    )
    return out


def swiglu_rows(rows, gate, upward):
    gate_part = jnp.dot(rows, gate, preferred_element_type=jnp.float32)
    up_part = jnp.dot(rows, upward, preferred_element_type=jnp.float32)
    return (jax.nn.silu(gate_part) * up_part).astype(jnp.bfloat16)


def plain_device(
    tokens,
    routes,
    route_weights,
    norm_gain,
    expert_gate,
    expert_up,
    expert_down,
    shared_gate,
    shared_up,
    shared_down,
    out_gain,
):
    count_tokens, width = tokens.shape
    top_count = routes.shape[1]
    experts = lax.axis_size("ep")
    capacity = max(2, 3 * count_tokens * top_count // (2 * experts))
    tokens_f32 = tokens.astype(jnp.float32)
    inverse = lax.rsqrt(jnp.mean(tokens_f32 * tokens_f32, axis=1, keepdims=True) + 1e-06)
    normed = (tokens_f32 * inverse * norm_gain[None, :]).astype(jnp.bfloat16)
    chosen = routes.reshape(-1)
    marks = (chosen[:, None] == jnp.arange(experts, dtype=jnp.int32)[None, :]).astype(jnp.int32)
    slots = jnp.sum(jnp.cumsum(marks, axis=0) * marks, axis=1) - 1
    places = chosen * capacity + slots
    owners = jnp.arange(chosen.shape[0], dtype=jnp.int32) // top_count
    table = jnp.zeros((experts * capacity,), jnp.int32).at[places].set(owners)
    filled = jnp.zeros((experts * capacity,), jnp.bool_).at[places].set(True)
    outbound = jnp.where(filled[:, None], normed[table], jnp.zeros((), jnp.bfloat16))
    outbound = outbound.reshape(experts, capacity, width)
    arrived = lax.all_to_all(outbound, "ep", split_axis=0, concat_axis=0, tiled=True).reshape(
        experts * capacity, width
    )
    hidden = swiglu_rows(arrived, expert_gate[0], expert_up[0])
    results = jnp.dot(
        hidden,
        lax.all_gather(expert_down[0], "tp", axis=1, tiled=True),
        preferred_element_type=jnp.float32,
    ).astype(jnp.bfloat16)
    returned = lax.all_to_all(
        results.reshape(experts, capacity, width), "ep", split_axis=0, concat_axis=0, tiled=True
    )
    returned = returned.reshape(experts * capacity, width)
    picked = returned[places].astype(jnp.float32).reshape(count_tokens, top_count, width)
    routed = jnp.sum(picked * route_weights[:, :, None], axis=1)
    shared_hidden = swiglu_rows(normed, shared_gate, shared_up)
    shared_out = jnp.dot(
        shared_hidden,
        lax.all_gather(shared_down, "tp", axis=1, tiled=True),
        preferred_element_type=jnp.float32,
    )
    moe = (shared_out + routed).astype(jnp.bfloat16)
    columns = lax.all_to_all(moe, "tp", split_axis=1, concat_axis=0, tiled=True)
    values = columns.astype(jnp.float32)
    own_rows = moe.astype(jnp.float32)
    totals = lax.all_gather(jnp.sum(own_rows * own_rows, axis=1), "tp", axis=0, tiled=True)
    scale = lax.rsqrt(totals / width + 1e-06)
    return (values * scale[:, None] * out_gain[None, :]).astype(jnp.bfloat16)


def per_device(tokens, routes, *rest):
    count, width = tokens.shape
    experts, blocks = lax.axis_size("ep"), lax.axis_size("tp")
    capacity = 3 * count * routes.shape[1] // (2 * experts)
    powers = experts & (experts - 1) == 0 and blocks & (blocks - 1) == 0
    aligned = capacity % 16 == 0 and width // blocks % 128 == 0 and count % 128 == 0
    fits = powers and aligned and experts >= 8
    return (fast_device if fits else plain_device)(tokens, routes, *rest)


def solution(mesh):
    in_specs = (
        P(("ep", "tp"), None),
        P(("ep", "tp"), None),
        P(("ep", "tp"), None),
        P(),
        P("ep", None, None),
        P("ep", None, None),
        P("ep", None, "tp"),
        P(),
        P(),
        P(None, "tp"),
        P("tp"),
    )
    out_specs = P("ep", "tp")
    return jax.shard_map(
        per_device, mesh=mesh, in_specs=in_specs, out_specs=out_specs, check_vma=False
    )
```

```python
import functools

import jax
import jax.numpy as jnp
from jax import lax
from jax.experimental import pallas as pl
from jax.experimental.pallas import tpu as pltpu
from jax.sharding import PartitionSpec as P


VMEM = pl.BlockSpec(memory_space=pltpu.VMEM)
SMEM = pl.BlockSpec(memory_space=pltpu.SMEM)
HBM = pl.BlockSpec(memory_space=pltpu.HBM)
F32 = jnp.float32
CHUNKS = 1
BF16 = jnp.bfloat16


def dot(a, b):
    return jnp.dot(a, b, preferred_element_type=F32)


def call(kernel, outs, inputs, flops, scalars=0, far=(), scratch=(), far_out=False):
    moved = sum(a.size * a.dtype.itemsize for a in inputs)
    moved += sum(o.size * o.dtype.itemsize for o in outs)
    specs = [SMEM] * scalars + [VMEM] * (len(inputs) - scalars)
    for i in far:
        specs[i] = HBM
        inputs[i] = pltpu.with_memory_space_constraint(inputs[i], pltpu.HBM)
    return pl.pallas_call(
        kernel,
        out_shape=outs,
        in_specs=specs,
        out_specs=[HBM if far_out else VMEM] * len(outs),
        scratch_shapes=scratch,
        cost_estimate=pl.CostEstimate(flops=flops, bytes_accessed=moved, transcendentals=0),
        compiler_params=pltpu.CompilerParams(vmem_limit_bytes=40 * 1024 * 1024),
    )(*inputs)


def fetch(sources, targets, sems):
    copies = [
        pltpu.make_async_copy(source, target, sems.at[i])
        for i, (source, target) in enumerate(zip(sources, targets))
    ]
    for copy in copies:
        copy.start()
    return copies


def swiglu(rows, both):
    parts = dot(rows, both)
    inner = parts.shape[1] // 2
    gate_part, up_part = parts[:, :inner], parts[:, inner:]
    return (gate_part / (1.0 + jnp.exp(-gate_part)) * up_part).astype(BF16)


def normalize(values, gain):
    values = values.astype(F32)
    inverse = lax.rsqrt(jnp.mean(values * values, axis=1, keepdims=True) + 1e-06)
    return (values * inverse * gain).astype(BF16)


def places_of(me, routes, capacity, experts):
    count = routes.shape[1]
    index = lax.broadcasted_iota(jnp.int32, (experts, count), 0)
    rows = [routes[j : j + 1, :] for j in range(routes.shape[0])]
    marks = [index == row for row in rows]
    marked = functools.reduce(jnp.logical_or, marks)
    earlier = lax.broadcasted_iota(jnp.int32, (count, count), 0) < lax.broadcasted_iota(
        jnp.int32, (count, count), 1
    )
    before = dot(marked.astype(BF16), earlier.astype(BF16))
    places = []
    for row, mark in zip(rows, marks):
        slot = jnp.sum(jnp.where(mark, before, 0.0), axis=0, keepdims=True)
        places.append((row ^ me) * capacity + slot.astype(jnp.int32))
    return places


def picks(places, first, units, capacity):
    shape = (units * capacity, places[0].shape[1])
    at = lax.broadcasted_iota(jnp.int32, shape, 0) + first * capacity
    chosen = functools.reduce(jnp.logical_or, [at == place for place in places])
    return chosen.astype(F32).astype(BF16)


def prepare_kernel(experts, capacity, first, chunks, me, tokens, routes, held, kept, *refs):
    pieces, sems = refs[:-1], refs[-1]
    step = tokens.shape[1] // chunks
    spans = [pl.ds(c * step, step) for c in range(chunks)]
    sources = [routes] + [tokens.at[:, span] for span in spans]
    copies = fetch(sources, [kept] + [held.at[:, span] for span in spans], sems)
    copies[0].wait()
    chosen = picks(places_of(me[0], kept, capacity, experts), first, len(pieces), capacity)
    for copy, span in zip(copies[1:], spans):
        copy.wait()
        moved = dot(chosen, held[:, span]).astype(BF16)
        for u, piece in enumerate(pieces):
            piece[:, span] = moved[u * capacity : (u + 1) * capacity]


def remain_kernel(experts, capacity, groups, me, held, kept, *pieces):
    places = places_of(me[0], kept, capacity, experts)
    done = 0
    for first, units in groups:
        moved = dot(picks(places, first, units, capacity), held[...]).astype(BF16)
        for u in range(units):
            pieces[done + u][...] = moved[u * capacity : (u + 1) * capacity]
        done += units


def table_kernel(capacity, groups, me, *refs):
    packed, outs = refs[: -len(groups)], refs[-len(groups) :]
    for m, ref in enumerate(packed):
        top_count = ref.shape[0] // 2
        count = ref.shape[1]
        columns = [
            jnp.broadcast_to(ref[r : r + 1, :], (count, count)).T for r in range(2 * top_count)
        ]
        lane = lax.broadcasted_iota(jnp.int32, (count, count), 1)
        chosen = [c.astype(jnp.int32) for c in columns[:top_count]]
        marks = [lane == c for c in chosen]
        marked = functools.reduce(jnp.logical_or, marks)
        earlier = lax.broadcasted_iota(jnp.int32, (count, count), 0) > lane
        before = dot(earlier.astype(F32).astype(BF16), marked.astype(F32).astype(BF16))
        places = []
        for c, mark in zip(chosen, marks):
            slot = jnp.sum(jnp.where(mark, before, 0.0), axis=1, keepdims=True)
            places.append((c[:, :1] ^ me[0]) * capacity + slot.astype(jnp.int32))
        for (start, size), out in zip(groups, outs):
            wide = size * capacity
            at = lax.broadcasted_iota(jnp.int32, (count, wide), 1) + start * capacity
            table = functools.reduce(
                jnp.add,
                [
                    jnp.where(at == place, weight[:, :1], 0.0)
                    for place, weight in zip(places, columns[top_count:])
                ],
            )
            parts = []
            for _ in range(3):
                piece = table.astype(BF16)
                parts.append(piece)
                table = table - piece.astype(F32)
            out[m] = jnp.concatenate(parts, axis=1)


def stage_kernel(gate, upward, held, both, sems):
    inner = gate.shape[1]
    for copy in fetch((gate, upward), (both.at[:, :inner], both.at[:, inner:]), sems):
        copy.wait()


def shared_kernel(tokens, gain, gate, upward, hidden, both, sems):
    inner = gate.shape[1]
    copies = fetch((gate, upward), (both.at[:, :inner], both.at[:, inner:]), sems)
    rows = normalize(tokens[...], gain[...])
    for copy in copies:
        copy.wait()
    hidden[...] = swiglu(rows, both[...])


def hidden_kernel(*refs):
    gain, both, out = refs[-3:]
    rows = jnp.concatenate([r[...] for r in refs[:-3]], axis=0)
    out[...] = swiglu(normalize(rows, gain[...]), both[...])


def down_kernel(blocks, units, capacity, *refs):
    hidden = refs[:blocks]
    down = refs[blocks]
    outs = refs[blocks + 1 :]
    count = units * capacity
    rows = jnp.concatenate([h[...] for h in hidden], axis=0)
    result = dot(rows, down[...]).astype(BF16)
    for u in range(units):
        for m in range(blocks):
            first = m * count + u * capacity
            outs[u][m] = result[first : first + capacity]


def weighted(table, returned, m):
    rows = jnp.concatenate([r[m] for r in returned], axis=0)
    return dot(table[m], jnp.concatenate([rows] * 3, axis=0))


def base_kernel(blocks, *refs):
    hidden = refs[:blocks]
    down, table = refs[blocks : blocks + 2]
    returned, out = refs[blocks + 2 : -1], refs[-1]
    shared = dot(jnp.concatenate([h[...] for h in hidden], axis=0), down[...])
    count = out.shape[1]
    for m in range(blocks):
        out[m] = shared[m * count : (m + 1) * count] + weighted(table, returned, m)


def more_kernel(blocks, total, table, *refs):
    for m in range(blocks):
        refs[-1][m] = total[m] + weighted(table, refs[:-1], m)


def finish_kernel(blocks, total, table, *refs):
    returned = refs[:-2]
    moe, squares = refs[-2:]
    count = moe.shape[1]
    lane = lax.broadcasted_iota(jnp.int32, (count, count), 1)
    sums = jnp.zeros((count, count), F32)
    for m in range(blocks):
        rounded = (total[m] + weighted(table, returned, m)).astype(BF16)
        moe[m] = rounded
        wide = rounded.astype(F32)
        sums = jnp.where(lane == m, jnp.sum(wide * wide, axis=1, keepdims=True), sums)
    squares[...] = sums.T[:blocks, :]


def scale_kernel(blocks, width, me, moe, gain, *refs):
    squares, out, ready, sems = refs[:blocks], *refs[blocks:]
    count = moe.shape[1]
    totals = []
    for m in range(blocks):
        total = squares[0][m : m + 1, :]
        for p in range(1, blocks):
            total = total + squares[p][m ^ p : (m ^ p) + 1, :]
        totals.append(lax.rsqrt(total / width + 1e-06))
    totals.append(jnp.zeros((count - blocks, count), F32))
    columns = jnp.concatenate(totals, axis=0).T
    copies = []
    for m in range(blocks):
        column = columns[:, m : m + 1]
        ready[m] = (moe[m].astype(F32) * column * gain[...]).astype(BF16)
        first = pl.multiple_of((me[0] ^ m) * count, count)
        copy = pltpu.make_async_copy(ready.at[m], out.at[pl.ds(first, count), :], sems.at[m])
        copy.start()
        copies.append(copy)
    for copy in copies:
        copy.wait()


def swap(array, axis, k):
    size = lax.axis_size(axis)
    return lax.ppermute(array, axis, [(s, s ^ k) for s in range(size)])


def spread(array):
    return [array] + [swap(array, "tp", m) for m in range(1, lax.axis_size("tp"))]


def fast_device(
    tokens,
    routes,
    route_weights,
    norm_gain,
    expert_gate,
    expert_up,
    expert_down,
    shared_gate,
    shared_up,
    shared_down,
    out_gain,
):
    count, width = tokens.shape
    top_count = routes.shape[1]
    experts = lax.axis_size("ep")
    blocks = lax.axis_size("tp")
    inner = expert_gate.shape[2]
    local = expert_down.shape[2]
    capacity = 3 * count * top_count // (2 * experts)
    row = lax.axis_index("ep").astype(jnp.int32).reshape(1)
    column = lax.axis_index("tp").astype(jnp.int32).reshape(1)
    piece = jax.ShapeDtypeStruct((capacity, width), BF16)
    gain = norm_gain[None, :]
    half, quarter = experts // 2, experts // 4
    held, kept, *pieces = call(
        functools.partial(prepare_kernel, experts, capacity, half + quarter, CHUNKS),
        [
            jax.ShapeDtypeStruct((count, width), BF16),
            jax.ShapeDtypeStruct((top_count, count), jnp.int32),
        ]
        + [piece] * quarter,
        [row, tokens, routes.T],
        2 * quarter * capacity * count * width,
        scalars=1,
        far=(1, 2),
        scratch=[pltpu.SemaphoreType.DMA((1 + CHUNKS,))],
    )
    rest = call(
        functools.partial(
            remain_kernel, experts, capacity, [(0, half), (half, quarter)]
        ),
        [piece] * (experts - quarter),
        [row, held, kept],
        2 * (experts - quarter) * capacity * count * width,
        scalars=1,
    )
    pieces = [*rest, *pieces]
    arrived = [pieces[0]] + [swap(pieces[k], "ep", k) for k in range(1, experts)]
    groups = {"N": (0, half), "A": (half + quarter, quarter), "B": (half, quarter)}

    packed = jnp.concatenate([routes.T.astype(F32), route_weights.T], axis=0)
    packed = spread(packed)
    both = jax.ShapeDtypeStruct((width, 2 * inner), BF16)
    (weights,) = call(
        stage_kernel,
        [both],
        [expert_gate[0], expert_up[0], pieces[0]],
        count * width,
        far=(0, 1),
        scratch=[pltpu.SemaphoreType.DMA((2,))],
    )
    (shared,) = call(
        shared_kernel,
        [jax.ShapeDtypeStruct((count, inner), BF16)],
        [tokens, gain, shared_gate, shared_up],
        4 * count * width * inner,
        far=(2, 3),
        scratch=[pltpu.VMEM(both.shape, BF16), pltpu.SemaphoreType.DMA((2,))],
    )
    shared = spread(shared)
    tables = call(
        functools.partial(table_kernel, capacity, list(groups.values())),
        [
            jax.ShapeDtypeStruct((blocks, count, 3 * size * capacity), BF16)
            for _, size in groups.values()
        ],
        [row] + packed,
        blocks * count * count * count,
        scalars=1,
    )

    returned = {}
    for name, (first, size) in groups.items():
        rows = size * capacity
        (hidden,) = call(
            hidden_kernel,
            [jax.ShapeDtypeStruct((rows, inner), BF16)],
            arrived[first : first + size] + [gain, weights],
            4 * rows * width * inner,
        )
        results = call(
            functools.partial(down_kernel, blocks, size, capacity),
            [jax.ShapeDtypeStruct((blocks, capacity, local), BF16)] * size,
            spread(hidden) + [expert_down[0]],
            2 * blocks * rows * inner * local,
        )
        returned[name] = [
            swap(results[u], "ep", first + u) if first + u else results[u]
            for u in range(size)
        ]

    sums = jax.ShapeDtypeStruct((blocks, count, local), F32)
    (total,) = call(
        functools.partial(base_kernel, blocks),
        [sums],
        shared + [shared_down, tables[1]] + returned["A"],
        2 * blocks * count * local * (inner + 3 * quarter * capacity),
    )
    (total,) = call(
        functools.partial(more_kernel, blocks),
        [sums],
        [total, tables[0]] + returned["N"],
        2 * blocks * count * local * 3 * half * capacity,
    )
    moe, squares = call(
        functools.partial(finish_kernel, blocks),
        [
            jax.ShapeDtypeStruct((blocks, count, local), BF16),
            jax.ShapeDtypeStruct((blocks, count), F32),
        ],
        [total, tables[2]] + returned["B"],
        2 * blocks * count * local * 3 * quarter * capacity,
    )
    (out,) = call(
        functools.partial(scale_kernel, blocks, width),
        [jax.ShapeDtypeStruct((blocks * count, local), BF16)],
        [column, moe, out_gain[None, :]] + spread(squares),
        4 * blocks * count * local,
        scalars=1,
        scratch=[
            pltpu.VMEM((blocks, count, local), BF16),
            pltpu.SemaphoreType.DMA((blocks,)),
        ],
        far_out=True,
    )
    return out


def swiglu_rows(rows, gate, upward):
    gate_part = jnp.dot(rows, gate, preferred_element_type=jnp.float32)
    up_part = jnp.dot(rows, upward, preferred_element_type=jnp.float32)
    return (jax.nn.silu(gate_part) * up_part).astype(jnp.bfloat16)


def plain_device(
    tokens,
    routes,
    route_weights,
    norm_gain,
    expert_gate,
    expert_up,
    expert_down,
    shared_gate,
    shared_up,
    shared_down,
    out_gain,
):
    count_tokens, width = tokens.shape
    top_count = routes.shape[1]
    experts = lax.axis_size("ep")
    capacity = max(2, 3 * count_tokens * top_count // (2 * experts))
    tokens_f32 = tokens.astype(jnp.float32)
    inverse = lax.rsqrt(jnp.mean(tokens_f32 * tokens_f32, axis=1, keepdims=True) + 1e-06)
    normed = (tokens_f32 * inverse * norm_gain[None, :]).astype(jnp.bfloat16)
    chosen = routes.reshape(-1)
    marks = (chosen[:, None] == jnp.arange(experts, dtype=jnp.int32)[None, :]).astype(jnp.int32)
    slots = jnp.sum(jnp.cumsum(marks, axis=0) * marks, axis=1) - 1
    places = chosen * capacity + slots
    owners = jnp.arange(chosen.shape[0], dtype=jnp.int32) // top_count
    table = jnp.zeros((experts * capacity,), jnp.int32).at[places].set(owners)
    filled = jnp.zeros((experts * capacity,), jnp.bool_).at[places].set(True)
    outbound = jnp.where(filled[:, None], normed[table], jnp.zeros((), jnp.bfloat16))
    outbound = outbound.reshape(experts, capacity, width)
    arrived = lax.all_to_all(outbound, "ep", split_axis=0, concat_axis=0, tiled=True).reshape(
        experts * capacity, width
    )
    hidden = swiglu_rows(arrived, expert_gate[0], expert_up[0])
    results = jnp.dot(
        hidden,
        lax.all_gather(expert_down[0], "tp", axis=1, tiled=True),
        preferred_element_type=jnp.float32,
    ).astype(jnp.bfloat16)
    returned = lax.all_to_all(
        results.reshape(experts, capacity, width), "ep", split_axis=0, concat_axis=0, tiled=True
    )
    returned = returned.reshape(experts * capacity, width)
    picked = returned[places].astype(jnp.float32).reshape(count_tokens, top_count, width)
    routed = jnp.sum(picked * route_weights[:, :, None], axis=1)
    shared_hidden = swiglu_rows(normed, shared_gate, shared_up)
    shared_out = jnp.dot(
        shared_hidden,
        lax.all_gather(shared_down, "tp", axis=1, tiled=True),
        preferred_element_type=jnp.float32,
    )
    moe = (shared_out + routed).astype(jnp.bfloat16)
    columns = lax.all_to_all(moe, "tp", split_axis=1, concat_axis=0, tiled=True)
    values = columns.astype(jnp.float32)
    own_rows = moe.astype(jnp.float32)
    totals = lax.all_gather(jnp.sum(own_rows * own_rows, axis=1), "tp", axis=0, tiled=True)
    scale = lax.rsqrt(totals / width + 1e-06)
    return (values * scale[:, None] * out_gain[None, :]).astype(jnp.bfloat16)


def per_device(tokens, routes, *rest):
    count, width = tokens.shape
    experts, blocks = lax.axis_size("ep"), lax.axis_size("tp")
    capacity = 3 * count * routes.shape[1] // (2 * experts)
    powers = experts & (experts - 1) == 0 and blocks & (blocks - 1) == 0
    aligned = capacity % 16 == 0 and width // blocks % 128 == 0 and count % 128 == 0
    fits = powers and aligned and experts >= 8
    return (fast_device if fits else plain_device)(tokens, routes, *rest)


def solution(mesh):
    in_specs = (
        P(("ep", "tp"), None),
        P(("ep", "tp"), None),
        P(("ep", "tp"), None),
        P(),
        P("ep", None, None),
        P("ep", None, None),
        P("ep", None, "tp"),
        P(),
        P(),
        P(None, "tp"),
        P("tp"),
    )
    out_specs = P("ep", "tp")
    return jax.shard_map(
        per_device, mesh=mesh, in_specs=in_specs, out_specs=out_specs, check_vma=False
    )
```
